32 devices in a mesh: fs: 8 (over z, x), tp: 4 (over y, core).
Axes of the slice: x: 2, y: 2, z: 4, core: 2. Of those that a mesh axis runs over, the one named last changes fastest.
Arguments:
- saved_input: bfloat16 [2048, 4096], P('fs'), may hold values from -8 to 8
- query_cotangent: bfloat16 [2048, 2048], P('fs', 'tp'), may hold values from -6 to 6
- layer_cotangent: bfloat16 [2048, 4096], P('fs'), may hold values from -8 to 8
- mixed_heads: bfloat16 [2048, 2048], P('fs', 'tp'), may hold values from -6 to 6
- query_basis: bfloat16 [4096, 256], P('fs'), may hold values from -0.125 to 0.125
- output_basis: bfloat16 [4096, 256], P('fs'), may hold values from -0.125 to 0.125
- query_master: float32 [4096, 2048], P('fs', 'tp'), may hold values from -3 to 3
- output_master: float32 [4096, 2048], P('fs', 'tp'), may hold values from -3 to 3
- query_first: float32 [256, 2048], P('fs', 'tp'), may hold values from -6 to 6
- query_second: float32 [256, 2048], P('fs', 'tp'), may hold values from 0.25 to 4
- output_first: float32 [256, 2048], P('fs', 'tp'), may hold values from -6 to 6
- output_second: float32 [256, 2048], P('fs', 'tp'), may hold values from 0.25 to 4
Outputs:
- query_weight: float32 [4096, 2048], P('fs', 'tp')
- output_weight: float32 [4096, 2048], P('fs', 'tp')
- query_step: float32 [4096, 2048], P('fs', 'tp')
- output_step: float32 [4096, 2048], P('fs', 'tp')
- query_first_new: float32 [256, 2048], P('fs', 'tp')
- query_second_new: float32 [256, 2048], P('fs', 'tp')
- output_first_new: float32 [256, 2048], P('fs', 'tp')
- output_second_new: float32 [256, 2048], P('fs', 'tp')
- query_copy: bfloat16 [4096, 2048], P(None, 'tp')
- output_copy: bfloat16 [4096, 2048], P(None, 'tp')
The draws below stay inside these ranges and needn't reach their ends.
All inputs are finite; a program needn't handle non-finite values.
Results may differ from the reference program's by a relative error of at most 0.0028.
Values may be sent and summed in bfloat16 or wider, within the bound.
A program may use at most 64 MiB of HBM per device.

```python
import math
import jax
import jax.numpy as jnp
from jax import lax

D = 4096
QW = 2048
RANK = 256
TOKENS = 2048


def with_spikes(values, rng, source, target, parts, factor):
    owner, partner = [(jnp.arange(values.shape[axis_at]) // (values.shape[axis_at] // parts)).reshape([-1 if axis == axis_at else 1 for axis in range(values.ndim)]) for axis_at in (source, target)]
    chosen = jax.random.permutation(rng, parts)[partner]
    strong = (owner == chosen) | (owner == (partner + parts // 2) % parts)
    return jnp.where(strong, factor * values, values)


def block_scale(rng, dims, shards, smallest, high):
    factor_of, own = 1.0, jax.random.fold_in(rng, 6)
    for dim, shards_of in shards:
        draws = jnp.exp(jax.random.uniform(jax.random.fold_in(own, dim), (shards_of,), jnp.float32, smallest / len(shards), high / len(shards)))
        factor_of = factor_of * jnp.repeat(draws, dims[dim] // shards_of).reshape([-1 if axis == dim else 1 for axis in range(len(dims))])
    return factor_of


def centred(stream_key, shape, scale, reach, shards=(), kind=jnp.bfloat16):
    drawn = scale * jax.random.normal(stream_key, shape, jnp.float32)
    if shards:
        drawn = drawn * block_scale(stream_key, shape, shards, -0.22, 0.18)
    return jnp.clip(drawn, -reach, reach).astype(kind)


def bell_draw_with(rng, shape, spread, limit, cuts, heavy, held_as=jnp.bfloat16):
    values = spread * jax.random.normal(rng, shape, jnp.float32)
    if cuts:
        values = values * block_scale(rng, shape, cuts, -0.22, 0.18)
    return jnp.clip(with_spikes(values, jax.random.fold_in(rng, 3), *heavy), -limit, limit).astype(held_as)


def setup_inputs(seed: int = 0) -> dict:
    key_of = jax.random.split(jax.random.key(seed), 13)
    saved_input = bell_draw_with(key_of[0], (TOKENS, D), 1.0, 8.0, ((0, 8),), (0, 1, 8, 2.0))
    query_cotangent = centred(key_of[1], (TOKENS, QW), 1.0, 6.0, ((0, 8), (1, 4)))
    layer_cotangent = bell_draw_with(key_of[2], (TOKENS, D), 1.0, 8.0, ((0, 8),), (0, 1, 8, 2.0))
    mixed_heads = centred(key_of[3], (TOKENS, QW), 1.0, 6.0, ((0, 8), (1, 4)))
    query_basis = bell_draw_with(key_of[4], (D, RANK), D ** -0.5, 0.125, ((0, 8),), (0, 1, 8, 2.0))
    output_basis = bell_draw_with(key_of[5], (D, RANK), D ** -0.5, 0.125, ((0, 8),), (0, 1, 8, 2.0))
    query_master = centred(key_of[6], (D, QW), 0.5, 3.0, ((0, 8), (1, 4)), jnp.float32)
    output_master = centred(key_of[7], (D, QW), 0.5, 3.0, ((0, 8), (1, 4)), jnp.float32)
    query_first = centred(key_of[8], (RANK, QW), 1.0, 6.0, ((0, 8), (1, 4)), jnp.float32)
    query_second = jnp.clip(jnp.exp(math.log(4.0) - 2.7725887 * jax.random.uniform(key_of[9], (RANK, QW), jnp.float32) ** block_scale(key_of[9], (RANK, QW), ((0, 8), (1, 4)), -0.2, 0.2)), 0.25, 4.0)
    output_first = centred(key_of[10], (RANK, QW), 1.0, 6.0, ((0, 8), (1, 4)), jnp.float32)
    output_second = jnp.clip(jnp.exp(math.log(4.0) - 2.7725887 * jax.random.uniform(key_of[11], (RANK, QW), jnp.float32) ** block_scale(key_of[11], (RANK, QW), ((0, 8), (1, 4)), -0.2, 0.2)), 0.25, 4.0)
    return dict(saved_input=saved_input, query_cotangent=query_cotangent, layer_cotangent=layer_cotangent, mixed_heads=mixed_heads, query_basis=query_basis, output_basis=output_basis, query_master=query_master, output_master=output_master, query_first=query_first, query_second=query_second, output_first=output_first, output_second=output_second)


beta_one = 0.8
beta_two = 0.9
rate = 0.1

def projected_gradient(saved, cotangent, basis):
    gradient = jnp.dot(saved.T, cotangent, preferred_element_type=jnp.float32)
    return jnp.dot(basis.astype(jnp.float32).T, gradient, precision=lax.Precision.HIGHEST)

def moment_update(low, factor, first, second):
    scaled = low * factor
    first_new = beta_one * first + (1.0 - beta_one) * scaled
    second_new = beta_two * second + (1.0 - beta_two) * scaled * scaled
    direction = (first_new / jnp.sqrt(second_new)).astype(jnp.bfloat16)
    return (first_new, second_new, direction)

def reference(saved_input, query_cotangent, layer_cotangent, mixed_heads, query_basis, output_basis, query_master, output_master, query_first, query_second, output_first, output_second):
    query_low = projected_gradient(saved_input, query_cotangent, query_basis)
    output_low = projected_gradient(layer_cotangent, mixed_heads, output_basis)
    meansq = (jnp.sum(query_low * query_low) + jnp.sum(output_low * output_low)) / (2.0 * RANK * QW)
    factor = 1.0 / jnp.sqrt(1.0 + meansq)
    qf, qs, qdir = moment_update(query_low, factor, query_first, query_second)
    of, osec, odir = moment_update(output_low, factor, output_first, output_second)
    query_step = jnp.dot(query_basis, qdir, preferred_element_type=jnp.float32)
    output_step = jnp.dot(output_basis, odir, preferred_element_type=jnp.float32)
    query_weight = query_master - rate * query_step
    output_weight = output_master - rate * output_step
    return (query_weight, output_weight, query_step, output_step, qf, qs, of, osec, query_weight.astype(jnp.bfloat16), output_weight.astype(jnp.bfloat16))
```

```python
import functools

import jax
import jax.numpy as jnp
from jax import lax
from jax.experimental import pallas as pl
from jax.experimental.pallas import tpu as pltpu
from jax.sharding import PartitionSpec as P

QW = 2048
RANK = 256


beta_one = 0.8
beta_two = 0.9
rate = 0.1


def moment_update(low, factor, first, second):
    scaled = low * factor
    first_new = beta_one * first + (1.0 - beta_one) * scaled
    second_new = beta_two * second + (1.0 - beta_two) * scaled * scaled
    direction = (first_new / jnp.sqrt(second_new)).astype(jnp.bfloat16)
    return (first_new, second_new, direction)


def contract_tokens(left, right):
    return lax.dot_general(
        left,
        right,
        (((0,), (0,)), ((), ())),
        precision=lax.Precision.HIGHEST,
        preferred_element_type=jnp.float32,
    )


def per_device(
    saved_input,
    query_cotangent,
    layer_cotangent,
    mixed_heads,
    query_basis,
    output_basis,
    query_master,
    output_master,
    query_first,
    query_second,
    output_first,
    output_second,
):
    query_coords = jnp.dot(
        saved_input,
        lax.all_gather(query_basis, "fs", axis=0, tiled=True),
        preferred_element_type=jnp.float32,
    )
    output_coords = jnp.dot(
        layer_cotangent,
        lax.all_gather(output_basis, "fs", axis=0, tiled=True),
        preferred_element_type=jnp.float32,
    )
    query_part = contract_tokens(query_coords, query_cotangent.astype(jnp.float32))
    output_part = contract_tokens(output_coords, mixed_heads.astype(jnp.float32))
    query_low, output_low = (
        lax.psum_scatter(query_part, "fs", scatter_dimension=0, tiled=True),
        lax.psum_scatter(output_part, "fs", scatter_dimension=0, tiled=True),
    )
    local_squares = jnp.sum(query_low * query_low) + jnp.sum(output_low * output_low)
    total_squares = lax.psum(local_squares, ("fs", "tp"))
    factor = 1.0 / jnp.sqrt(1.0 + total_squares / (2.0 * RANK * QW))
    qf, qs, qdir = moment_update(query_low, factor, query_first, query_second)
    of, osec, odir = moment_update(output_low, factor, output_first, output_second)
    query_whole, output_whole = (
        lax.all_gather(qdir, "fs", axis=0, tiled=True),
        lax.all_gather(odir, "fs", axis=0, tiled=True),
    )
    query_step = jnp.dot(query_basis, query_whole, preferred_element_type=jnp.float32)
    output_step = jnp.dot(output_basis, output_whole, preferred_element_type=jnp.float32)
    query_weight = query_master - rate * query_step
    output_weight = output_master - rate * output_step
    query_copy, output_copy = (
        lax.all_gather(query_weight.astype(jnp.bfloat16), "fs", axis=0, tiled=True),
        lax.all_gather(output_weight.astype(jnp.bfloat16), "fs", axis=0, tiled=True),
    )
    return (
        query_weight,
        output_weight,
        query_step,
        output_step,
        qf,
        qs,
        of,
        osec,
        query_copy,
        output_copy,
    )

MESH = pl.DeviceIdType.MESH
PIECES = 8
FLIGHT = 4
PACE = (4, 2, 2, 3, 3, 3, 3, 3, 3, 8, 6, 4)
STRETCH = 40.0
REACH = 3.0
LN2 = 0.6931471805599453


def encode(value):
    size = jnp.abs(value) * STRETCH
    small = size * LN2
    near = small * (1.0 + small * (0.5 + small * (1.0 / 6.0)))
    code = jnp.where(small < 0.02, near, jnp.exp2(size) - 1.0)
    return jnp.where(value < 0.0, -code, code).astype(jnp.bfloat16)


def decode(code):
    code = code.astype(jnp.float32)
    size = jnp.abs(code)
    near = size * (1.0 - size * (0.5 - size * (1.0 / 3.0)))
    value = jnp.where(size < 0.02, near, jnp.log(1.0 + size)) * (1.0 / (LN2 * STRETCH))
    return jnp.where(code < 0.0, -value, value)


def encode_scaled(value):
    peak = jnp.max(jnp.max(jnp.abs(value), axis=1, keepdims=True), axis=0, keepdims=True)
    unit = jnp.maximum(peak, 1e-30) * (1.0 / REACH)
    return encode(value / unit), unit


def ring_kernel(n, m, *refs):
    x_hbm, cot_hbm, basis_hbm, master_hbm, first_hbm, second_hbm = (
        (refs[0], refs[2]),
        (refs[1], refs[3]),
        (refs[4], refs[5]),
        (refs[6], refs[7]),
        (refs[8], refs[10]),
        (refs[9], refs[11]),
    )
    w_out, step_out, first_out, second_out, gathered = (
        (refs[12], refs[13]),
        (refs[14], refs[15]),
        (refs[16], refs[18]),
        (refs[17], refs[19]),
        (refs[20], refs[21]),
    )
    (
        x_v, cot_v, basis, master_v, first, second,
        rows_v, code_v, wide_v, flat_v, coord_v, part_v, mine_v, pair_v, sum_v, got_v, unit_v,
        square_v, direction_v,
        in_sem, rows_sem, coord_sem, pair_sem, part_sem, unit_sem, square_sem, direction_sem, ring_sem, wide_sem,
    ) = refs[22:]
    f, t = lax.axis_index("fs"), lax.axis_index("tp")
    me = f * m + t
    rank_part, block = rows_v.shape[2:]
    piece = block // PIECES
    rank = basis.shape[2]
    tokens = x_v.shape[1]
    columns = cot_v.shape[2]
    low_rows = first.shape[1]
    half = n // 2
    z, x = f // 2, lax.rem(f, 2)
    across = z * 2 + 1 - x
    partner, opposite = t + 1 - 2 * lax.rem(t, 2), lax.rem(t + m // 2, m)
    order = (1, half - 1, *range(2, half - 1))

    def along(d, side=None):
        side = x if side is None else side
        return lax.rem(z + d + half, half) * 2 + side

    def source_of(d):
        return along(-(d % half), x if d < half else 1 - x)

    loads = {}
    for i, (name, sources, target) in enumerate(
        (
            ("basis", basis_hbm, basis),
            ("master", master_hbm, master_v),
            ("x", x_hbm, x_v),
            ("cot", cot_hbm, cot_v),
            ("first", first_hbm, first),
            ("second", second_hbm, second),
        )
    ):
        for k in range(2):
            loads[name, k] = pltpu.make_async_copy(sources[k], target.at[k], in_sem.at[i, k])
    for copy in loads.values():
        copy.start()

    barrier = pltpu.get_barrier_semaphore()
    for d in range(1, n * m):
        other = lax.rem(me + d, n * m)
        pl.semaphore_signal(barrier, inc=1, device_id={"fs": other // m, "tp": lax.rem(other, m)}, device_id_type=MESH)

    chosen = lax.broadcasted_iota(jnp.int32, (rank_part, rank), 1) == (
        lax.broadcasted_iota(jnp.int32, (rank_part, rank), 0) + t * rank_part
    )
    select = jnp.where(chosen, 1.0, 0.0).astype(jnp.bfloat16)
    for k in range(2):
        loads["basis", k].wait()
        rows_v[k, 0] = lax.dot_general(
            select, basis[k], (((1,), (1,)), ((), ())), preferred_element_type=jnp.float32
        ).astype(jnp.bfloat16)
    with jax.named_scope("barrier"):
        pl.semaphore_wait(barrier, n * m - 1)

    sent = []

    def send(source, target, sems, index, device):
        copy = pltpu.make_async_remote_copy(
            src_ref=source,
            dst_ref=target,
            send_sem=sems.at[(0,) + index],
            recv_sem=sems.at[(1,) + index],
            device_id=device,
            device_id_type=MESH,
        )
        copy.start()
        sent.append(copy)
        return copy

    def push(own, slots, sems, k):
        copies = {half: send(own, slots(half), sems, (k, half), {"fs": across})}
        for d in order:
            copies[d] = send(own, slots(d), sems, (k, d), {"fs": along(d)})
        return copies

    def relay(copies, slots, sems, k):
        for d in order:
            with jax.named_scope(f"rows_wait#k={k}#d={d}"):
                copies[d].wait_recv()
            copies[half + d] = send(slots(d), slots(half + d), sems, (k, half + d), {"fs": across})

    place = (1 - x) * z + x * (n - 1 - z)

    def at(p):
        p = lax.rem(p + 2 * n, n)
        h = p // half
        return (1 - h) * 2 * p + h * (2 * (n - 1 - p) + 1)

    toward = (at(place + 1), at(place - 1))
    origin = [[at(place - s), at(place + s)] for s in range(n)]
    ring = {}
    slots = [
        (s, g * FLIGHT + w) for g in range(PIECES // FLIGHT) for s in range(n) for w in range(FLIGHT)
    ]
    arrived = []

    def advance(count):
        for _ in range(min(count, len(slots))):
            s, c = slots.pop(0)
            for k in range(2):
                if s > 0:
                    with jax.named_scope(f"ring_wait#s={s}#c={c}#k={k}"):
                        ring[s - 1, k, c].wait_recv()
                if s < n - 1:
                    where = code_v.at[k, origin[s][k], pl.ds(c * piece, piece)]
                    ring[s, k, c] = send(where, where, ring_sem, (k, s, c), {"fs": toward[k]})
            if s > 0:
                arrived.append((s, c))

    pace = list(PACE)

    def rows_at(k):
        return lambda d: rows_v.at[k, d]

    rows = [push(rows_v.at[k, 0], rows_at(k), rows_sem, k) for k in range(2)]
    for i in range(PIECES // FLIGHT):
        span = pl.ds(i * FLIGHT * piece, FLIGHT * piece)
        for k in range(2):
            if i == 0:
                loads["master", k].wait()
            code_v[k, f, span] = encode(master_v[k, span])
        if i == 0:
            advance(pace.pop(0))

    def coordinates(k, d):
        left = rows_v[k, d]
        right = x_v[k, :, pl.ds(pl.multiple_of(source_of(d) * block, block), block)]
        return lax.dot_general(left, right, (((1,), (1,)), ((), ())), preferred_element_type=jnp.float32)

    for k in range(2):
        relay(rows[k], rows_at(k), rows_sem, k)
        advance(pace.pop(0))
    coords = []
    for k in range(2):
        loads["x", k].wait()
        total = coordinates(k, 0)
        for d in range(1, half):
            total = total + coordinates(k, d)
        for d in range(half, n):
            with jax.named_scope(f"rows_late#k={k}#d={d}"):
                rows[k][d].wait_recv()
            total = total + coordinates(k, d)
        high = total.astype(jnp.bfloat16)
        coord_v[k, t, 0] = high
        coord_v[k, t, 1] = (total - high.astype(jnp.float32)).astype(jnp.bfloat16)
        coords.append(
            [
                send(coord_v.at[k, t], coord_v.at[k, t], coord_sem, (k, d), {"tp": lax.rem(t + d, m)})
                for d in range(1, m)
            ]
        )
        advance(pace.pop(0))

    wide = []
    for k in range(2):
        for target in (opposite, partner):
            index = (k, len(wide) % 2)
            wide.append(send(rows_v.at[k], wide_v.at[k, t], wide_sem, index, {"tp": target}))
        wide_v[k, t] = rows_v[k]
    pairs, units = [], []
    for k in range(2):
        loads["cot", k].wait()
        with jax.named_scope(f"coords_wait#k={k}"):
            for copy in coords[k]:
                copy.wait_recv()
        part = jnp.dot(
            coord_v[k, :, 0].reshape(rank, tokens), cot_v[k], preferred_element_type=jnp.float32
        ) + jnp.dot(coord_v[k, :, 1].reshape(rank, tokens), cot_v[k], preferred_element_type=jnp.float32)
        part_v[k] = part.reshape(n, low_rows, columns)
        code, unit = encode_scaled(part)
        mine_v[k] = code.reshape(n, low_rows, columns)
        unit_v[0, k, 0] = jnp.broadcast_to(unit, unit_v.shape[3:])
        pairs.append({})
        units.append({0: send(unit_v.at[0, k, 0], unit_v.at[1, k, 0], unit_sem, (k, 0), {"fs": across})})
        for d in (*order, 0):
            pairs[k][d] = send(
                mine_v.at[k, along(d, 1 - x)], pair_v.at[k, d], pair_sem, (k, d), {"fs": across}
            )
        advance(pace.pop(0))
    parts = []
    def paired(k, d):
        with jax.named_scope(f"pair_wait#k={k}#d={d}"):
            pairs[k][d].wait_recv()
        return decode(pair_v[k, d]) * unit_v[1, k, 0][:1, :1] + part_v[k, along(d)]

    for k in range(2):
        parts.append({})
        units[k][0].wait_recv()
        for d in order:
            code, unit = encode_scaled(paired(k, d))
            sum_v[k, d] = code
            unit_v[0, k, d] = jnp.broadcast_to(unit, unit_v.shape[3:])
            units[k][d] = send(unit_v.at[0, k, d], unit_v.at[1, k, d], unit_sem, (k, d), {"fs": along(d)})
            parts[k][d] = send(sum_v.at[k, d], got_v.at[k, d], part_sem, (k, d), {"fs": along(d)})
        advance(pace.pop(0))

    lows = []
    squares = jnp.zeros((), jnp.float32)
    for k in range(2):
        low = paired(k, 0)
        for d in range(1, half):
            with jax.named_scope(f"part_wait#k={k}#d={d}"):
                units[k][d].wait_recv()
                parts[k][d].wait_recv()
            low = low + decode(got_v[k, d]) * unit_v[1, k, d][:1, :1]
        lows.append(low)
        squares = squares + jnp.sum(low * low)
    square_v[0] = jnp.full(square_v.shape[1:], squares, jnp.float32)
    copies = []
    for d in range(1, n * m):
        other = lax.rem(me + d, n * m)
        copies.append(
            send(square_v.at[0], square_v.at[d], square_sem, (d,), {"fs": other // m, "tp": lax.rem(other, m)})
        )
    advance(pace.pop(0))
    for k in range(2):
        loads["first", k].wait()
        loads["second", k].wait()
    with jax.named_scope("square_wait"):
        for copy in copies:
            copy.wait_recv()
    total_squares = jnp.sum(square_v[...], axis=0)[:1, :1]
    factor = 1.0 / jnp.sqrt(1.0 + total_squares / (2.0 * rank * (columns * m)))

    directions = []
    for k in range(2):
        new_first, new_second, direction = moment_update(lows[k], factor, first[k], second[k])
        direction_v[k, f] = direction
        own = direction_v.at[k, f]
        directions.append(push(own, lambda d: own, direction_sem, k))
        first_out[k][...] = new_first
        second_out[k][...] = new_second
    advance(pace.pop(0))
    for k in range(2):
        wide[2 * k].wait_recv()
        there = wide_v.at[k, opposite]
        wide.append(send(there, there, wide_sem, (k, 2), {"tp": partner}))
    for k in range(2):
        for d in order:
            with jax.named_scope(f"direction_wait#k={k}#d={d}"):
                directions[k][d].wait_recv()
            there = direction_v.at[k, along(-d)]
            directions[k][half + d] = send(there, there, direction_sem, (k, half + d), {"fs": across})
    advance(pace.pop(0))
    with jax.named_scope("wide_wait"):
        for copy in (wide[1], wide[3], wide[4], wide[5]):
            copy.wait_recv()
    for k in range(2):
        for d in range(1, n):
            flat_v[k, source_of(d)] = wide_v[k, :, d].reshape(rank, block).T
    for k in range(2):
        for d in range(half, n):
            with jax.named_scope(f"direction_late#k={k}#d={d}"):
                directions[k][d].wait_recv()

    def own_rows(k, start, size):
        span = pl.ds(start, size)
        step = jnp.dot(
            basis[k, span, :], direction_v[k].reshape(rank, columns), preferred_element_type=jnp.float32
        )
        weight = master_v[k, span, :] - rate * step
        gathered[k][pl.ds(pl.multiple_of(f * block + start, size), size)] = weight.astype(jnp.bfloat16)
        step_out[k][span] = step
        w_out[k][span] = weight

    def finish(k, s, start, size):
        source = origin[s][k]
        span = pl.ds(start, size)
        step = jnp.dot(
            flat_v[k, source, span, :],
            direction_v[k].reshape(rank, columns),
            preferred_element_type=jnp.float32,
        )
        weight = decode(code_v[k, source, span]) - rate * step
        gathered[k][pl.ds(pl.multiple_of(source * block + start, size), size)] = weight.astype(jnp.bfloat16)

    own = [(k, i * FLIGHT * piece) for i in range(PIECES // FLIGHT) for k in range(2)]
    done = set()

    def ready(limit):
        for s in range(1, n):
            for g in range(PIECES // FLIGHT):
                if limit <= 0:
                    return
                if (s, g) in done or any((s, g * FLIGHT + w) not in arrived for w in range(FLIGHT)):
                    continue
                done.add((s, g))
                limit -= 1
                for k in range(2):
                    finish(k, s, g * FLIGHT * piece, FLIGHT * piece)

    while slots:
        last = slots[0] if slots[0][0] == n - 1 and slots[0][1] >= PIECES - FLIGHT else None
        advance(1)
        if last:
            for k in range(2):
                finish(k, last[0], last[1] * piece, piece)
            done.add((last[0], last[1] // FLIGHT))
        if own:
            k, start = own.pop(0)
            own_rows(k, start, FLIGHT * piece)
        else:
            ready(1)
    for k, start in own:
        own_rows(k, start, FLIGHT * piece)
    ready(n * PIECES)
    with jax.named_scope("drain"):
        for copy in sent:
            copy.wait_send()


def write_kernel(count, *refs):
    sem = refs[2 * count]
    copies = [pltpu.make_async_copy(refs[i], refs[count + i], sem.at[i]) for i in range(count)]
    for copy in copies:
        copy.start()
    for copy in copies:
        copy.wait()


def fused_per_device(n, m, *args):
    x, cot, _, _, basis = args[:5]
    first = args[8]
    block, rank = basis.shape
    columns = cot.shape[1]
    tokens, width = x.shape
    part = rank // m
    low_rows = first.shape[0]
    bf16, f32 = jnp.bfloat16, jnp.float32
    kinds = [((block, columns), f32)] * 4 + [(first.shape, f32)] * 4 + [((width, columns), bf16)] * 2
    hbm = pl.BlockSpec(memory_space=pltpu.HBM)
    vmem = pl.BlockSpec(memory_space=pltpu.VMEM)
    dma = pltpu.SemaphoreType.DMA
    results = pl.pallas_call(
        functools.partial(ring_kernel, n, m),
        out_shape=tuple(pltpu.VMEM(*kind) for kind in kinds),
        in_specs=[hbm] * 12,
        out_specs=(vmem,) * 10,
        scratch_shapes=[
            pltpu.VMEM((2, tokens, width), bf16),
            pltpu.VMEM((2, tokens, columns), bf16),
            pltpu.VMEM((2, block, rank), bf16),
            pltpu.VMEM((2, block, columns), f32),
            pltpu.VMEM((2, low_rows, columns), f32),
            pltpu.VMEM((2, low_rows, columns), f32),
            pltpu.VMEM((2, n, part, block), bf16),
            pltpu.VMEM((2, n, block, columns), bf16),
            pltpu.VMEM((2, m, n, part, block), bf16),
            pltpu.VMEM((2, n, block, rank), bf16),
            pltpu.VMEM((2, m, 2, part, tokens), bf16),
            pltpu.VMEM((2, n, low_rows, columns), f32),
            pltpu.VMEM((2, n, low_rows, columns), bf16),
            pltpu.VMEM((2, n // 2, low_rows, columns), bf16),
            pltpu.VMEM((2, n // 2, low_rows, columns), bf16),
            pltpu.VMEM((2, n // 2, low_rows, columns), bf16),
            pltpu.VMEM((2, 2, n // 2, 1, 128), f32),
            pltpu.VMEM((n * m, 1, 128), f32),
            pltpu.VMEM((2, n, low_rows, columns), bf16),
            dma((6, 2)),
            dma((2, 2, n)),
            dma((2, 2, m)),
            dma((2, 2, n // 2)),
            dma((2, 2, n // 2)),
            dma((2, 2, n // 2)),
            dma((2, n * m)),
            dma((2, 2, n)),
            dma((2, 2, n - 1, PIECES)),
            dma((2, 2, 3)),
        ],
        compiler_params=pltpu.CompilerParams(
            collective_id=0, has_side_effects=True, vmem_limit_bytes=48 * 2**20
        ),
    )(*args)
    return pl.pallas_call(
        functools.partial(write_kernel, len(kinds)),
        out_shape=tuple(jax.ShapeDtypeStruct(*kind) for kind in kinds),
        in_specs=[pl.BlockSpec(memory_space=pl.ANY)] * len(kinds),
        out_specs=(hbm,) * len(kinds),
        scratch_shapes=[dma((len(kinds),))],
        compiler_params=pltpu.CompilerParams(vmem_limit_bytes=2**20),
    )(*results)


def fits(n, m, *args):
    basis, first = args[4], args[8]
    return (
        n % 2 == 0
        and m == 4
        and basis.shape[1] // n % 16 == 0
        and basis.shape[1] // m % 16 == 0
        and basis.shape[0] // n % (16 * PIECES) == 0
        and basis.shape[0] // n % 128 == 0
        and first.shape[1] // m % 128 == 0
    )


def solution(mesh):
    placed = (
        P("fs", None),
        P("fs", "tp"),
        P("fs", None),
        P("fs", "tp"),
        P("fs", None),
        P("fs", None),
        P("fs", "tp"),
        P("fs", "tp"),
        P("fs", "tp"),
        P("fs", "tp"),
        P("fs", "tp"),
        P("fs", "tp"),
    )
    n, m = mesh.shape["fs"], mesh.shape["tp"]

    def step(*args):
        body = functools.partial(fused_per_device, n, m) if fits(n, m, *args) else per_device
        return jax.shard_map(
            body,
            mesh=mesh,
            in_specs=placed,
            out_specs=(P("fs", "tp"),) * 8 + (P(None, "tp"),) * 2,
            check_vma=False,
        )(*args)

    return step
```

```python
import functools

import jax
import jax.numpy as jnp
from jax import lax
from jax.experimental import pallas as pl
from jax.experimental.pallas import tpu as pltpu
from jax.sharding import PartitionSpec as P

QW = 2048
RANK = 256


beta_one = 0.8
beta_two = 0.9
rate = 0.1


def moment_update(low, factor, first, second):
    scaled = low * factor
    first_new = beta_one * first + (1.0 - beta_one) * scaled
    second_new = beta_two * second + (1.0 - beta_two) * scaled * scaled
    direction = (first_new / jnp.sqrt(second_new)).astype(jnp.bfloat16)
    return (first_new, second_new, direction)


def contract_tokens(left, right):
    return lax.dot_general(
        left,
        right,
        (((0,), (0,)), ((), ())),
        precision=lax.Precision.HIGHEST,
        preferred_element_type=jnp.float32,
    )


def per_device(
    saved_input,
    query_cotangent,
    layer_cotangent,
    mixed_heads,
    query_basis,
    output_basis,
    query_master,
    output_master,
    query_first,
    query_second,
    output_first,
    output_second,
):
    query_coords = jnp.dot(
        saved_input,
        lax.all_gather(query_basis, "fs", axis=0, tiled=True),
        preferred_element_type=jnp.float32,
    )
    output_coords = jnp.dot(
        layer_cotangent,
        lax.all_gather(output_basis, "fs", axis=0, tiled=True),
        preferred_element_type=jnp.float32,
    )
    query_part = contract_tokens(query_coords, query_cotangent.astype(jnp.float32))
    output_part = contract_tokens(output_coords, mixed_heads.astype(jnp.float32))
    query_low, output_low = (
        lax.psum_scatter(query_part, "fs", scatter_dimension=0, tiled=True),
        lax.psum_scatter(output_part, "fs", scatter_dimension=0, tiled=True),
    )
    local_squares = jnp.sum(query_low * query_low) + jnp.sum(output_low * output_low)
    total_squares = lax.psum(local_squares, ("fs", "tp"))
    factor = 1.0 / jnp.sqrt(1.0 + total_squares / (2.0 * RANK * QW))
    qf, qs, qdir = moment_update(query_low, factor, query_first, query_second)
    of, osec, odir = moment_update(output_low, factor, output_first, output_second)
    query_whole, output_whole = (
        lax.all_gather(qdir, "fs", axis=0, tiled=True),
        lax.all_gather(odir, "fs", axis=0, tiled=True),
    )
    query_step = jnp.dot(query_basis, query_whole, preferred_element_type=jnp.float32)
    output_step = jnp.dot(output_basis, output_whole, preferred_element_type=jnp.float32)
    query_weight = query_master - rate * query_step
    output_weight = output_master - rate * output_step
    query_copy, output_copy = (
        lax.all_gather(query_weight.astype(jnp.bfloat16), "fs", axis=0, tiled=True),
        lax.all_gather(output_weight.astype(jnp.bfloat16), "fs", axis=0, tiled=True),
    )
    return (
        query_weight,
        output_weight,
        query_step,
        output_step,
        qf,
        qs,
        of,
        osec,
        query_copy,
        output_copy,
    )

MESH = pl.DeviceIdType.MESH
PIECES = 8
FLIGHT = 8
PACE = (8, 2, 2, 3, 3, 3, 3, 3, 3, 6, 4, 4)
STRETCH = 40.0
REACH = 3.0
ROWS, COORD, WIDE, UNIT, PAIR, PART, SQUARE, DIRECTION, RING = range(9)
LN2 = 0.6931471805599453


def encode(value):
    size = jnp.abs(value) * STRETCH
    small = size * LN2
    near = small * (1.0 + small * (0.5 + small * (1.0 / 6.0)))
    code = jnp.where(small < 0.02, near, jnp.exp2(size) - 1.0)
    return jnp.where(value < 0.0, -code, code).astype(jnp.bfloat16)


def decode(code):
    code = code.astype(jnp.float32)
    size = jnp.abs(code)
    near = size * (1.0 - size * (0.5 - size * (1.0 / 3.0)))
    value = jnp.where(size < 0.02, near, jnp.log(1.0 + size)) * (1.0 / (LN2 * STRETCH))
    return jnp.where(code < 0.0, -value, value)


def encode_scaled(value):
    peak = jnp.max(jnp.max(jnp.abs(value), axis=1, keepdims=True), axis=0, keepdims=True)
    unit = jnp.maximum(peak, 1e-30) * (1.0 / REACH)
    return encode(value / unit), unit


def ring_kernel(n, m, *refs):
    x_hbm, cot_hbm, basis_hbm, master_hbm, first_hbm, second_hbm = (
        (refs[0], refs[2]),
        (refs[1], refs[3]),
        (refs[4], refs[5]),
        (refs[6], refs[7]),
        (refs[8], refs[10]),
        (refs[9], refs[11]),
    )
    w_out, step_out, first_out, second_out, gathered = (
        (refs[12], refs[13]),
        (refs[14], refs[15]),
        (refs[16], refs[18]),
        (refs[17], refs[19]),
        (refs[20], refs[21]),
    )
    (
        x_v, cot_v, basis, master_v, first, second,
        rows_v, code_v, wide_v, flat_v, coord_v, part_v, mine_v, pair_v, sum_v, got_v, unit_v,
        square_v, direction_v,
        in_sem, out_sem, square_sem, coord_sem, rows_sem, pair_sem, part_sem, unit_sem, direction_sem, ring_sem, wide_sem,
    ) = refs[22:]
    f, t = lax.axis_index("fs"), lax.axis_index("tp")
    me = f * m + t
    rank_part, block = rows_v.shape[2:]
    piece = block // PIECES
    rank = basis.shape[2]
    tokens = x_v.shape[1]
    columns = cot_v.shape[2]
    low_rows = first.shape[1]
    half = n // 2
    z, x = f // 2, lax.rem(f, 2)
    across = z * 2 + 1 - x
    partner, opposite = t + 1 - 2 * lax.rem(t, 2), lax.rem(t + m // 2, m)
    order = (1, half - 1, *range(2, half - 1))

    def along(d, side=None):
        side = x if side is None else side
        return lax.rem(z + d + half, half) * 2 + side

    def source_of(d):
        return along(-(d % half), x if d < half else 1 - x)

    loads = {}
    for i, (name, sources, target) in enumerate(
        (
            ("basis", basis_hbm, basis),
            ("master", master_hbm, master_v),
            ("x", x_hbm, x_v),
            ("cot", cot_hbm, cot_v),
            ("first", first_hbm, first),
            ("second", second_hbm, second),
        )
    ):
        for k in range(2):
            loads[name, k] = pltpu.make_async_copy(sources[k], target.at[k], in_sem.at[i, k])
    for copy in loads.values():
        copy.start()

    barrier = pltpu.get_barrier_semaphore()
    for d in range(1, n * m):
        other = lax.rem(me + d, n * m)
        pl.semaphore_signal(barrier, inc=1, device_id={"fs": other // m, "tp": lax.rem(other, m)}, device_id_type=MESH)

    chosen = lax.broadcasted_iota(jnp.int32, (rank_part, rank), 1) == (
        lax.broadcasted_iota(jnp.int32, (rank_part, rank), 0) + t * rank_part
    )
    select = jnp.where(chosen, 1.0, 0.0).astype(jnp.bfloat16)
    for k in range(2):
        loads["basis", k].wait()
        rows_v[k, 0] = lax.dot_general(
            select, basis[k], (((1,), (1,)), ((), ())), preferred_element_type=jnp.float32
        ).astype(jnp.bfloat16)
    with jax.named_scope("barrier"):
        pl.semaphore_wait(barrier, n * m - 1)

    def send(source, target, out, arrival, device):
        copy = pltpu.make_async_remote_copy(
            src_ref=source,
            dst_ref=target,
            send_sem=out_sem.at[out],
            recv_sem=arrival,
            device_id=device,
            device_id_type=MESH,
        )
        copy.start()
        return copy

    def wait_bytes(like, sem):
        pltpu.make_async_copy(like, like, sem).wait()

    def push(own, slots, out, sems, k):
        copies = {half: send(own, slots(half), (out, k), sems.at[k, half], {"fs": across})}
        for d in order:
            copies[d] = send(own, slots(d), (out, k), sems.at[k, d], {"fs": along(d)})
        return copies

    def relay(copies, slots, out, sems, k):
        for d in order:
            with jax.named_scope(f"rows_wait#k={k}#d={d}"):
                copies[d].wait_recv()
            copies[half + d] = send(slots(d), slots(half + d), (out, k), sems.at[k, half + d], {"fs": across})

    place = (1 - x) * z + x * (n - 1 - z)

    def at(p):
        p = lax.rem(p + 2 * n, n)
        h = p // half
        return (1 - h) * 2 * p + h * (2 * (n - 1 - p) + 1)

    toward = (at(place + 1), at(place - 1))
    origin = [[at(place - s), at(place + s)] for s in range(n)]
    ring = {}
    slots = [
        (s, g * FLIGHT + w) for g in range(PIECES // FLIGHT) for s in range(n) for w in range(FLIGHT)
    ]
    arrived = []

    def advance(count):
        for _ in range(min(count, len(slots))):
            s, c = slots.pop(0)
            for k in range(2):
                if s > 0:
                    with jax.named_scope(f"ring_wait#s={s}#c={c}#k={k}"):
                        ring[s - 1, k, c].wait_recv()
                if s < n - 1:
                    where = code_v.at[k, origin[s][k], pl.ds(c * piece, piece)]
                    ring[s, k, c] = send(where, where, (RING, k), ring_sem.at[k, s, c], {"fs": toward[k]})
            if s > 0:
                arrived.append((s, c))

    pace = list(PACE)

    def rows_at(k):
        return lambda d: rows_v.at[k, d]

    rows = [push(rows_v.at[k, 0], rows_at(k), ROWS, rows_sem, k) for k in range(2)]
    for i in range(PIECES // FLIGHT):
        span = pl.ds(i * FLIGHT * piece, FLIGHT * piece)
        for k in range(2):
            if i == 0:
                loads["master", k].wait()
            code_v[k, f, span] = encode(master_v[k, span])
        if i == 0:
            advance(pace.pop(0))

    def coordinates(k, d):
        left = rows_v[k, d]
        right = x_v[k, :, pl.ds(pl.multiple_of(source_of(d) * block, block), block)]
        return lax.dot_general(left, right, (((1,), (1,)), ((), ())), preferred_element_type=jnp.float32)

    for k in range(2):
        relay(rows[k], rows_at(k), ROWS, rows_sem, k)
        advance(pace.pop(0))
    for k in range(2):
        loads["x", k].wait()
        total = coordinates(k, 0)
        for d in range(1, half):
            total = total + coordinates(k, d)
        for d in range(half, n):
            with jax.named_scope(f"rows_late#k={k}#d={d}"):
                rows[k][d].wait_recv()
            total = total + coordinates(k, d)
        high = total.astype(jnp.bfloat16)
        coord_v[k, t, 0] = high
        coord_v[k, t, 1] = (total - high.astype(jnp.float32)).astype(jnp.bfloat16)
        for d in range(1, m):
            send(coord_v.at[k, t], coord_v.at[k, t], (COORD, k), coord_sem.at[k], {"tp": lax.rem(t + d, m)})
        advance(pace.pop(0))

    wide = []
    for k in range(2):
        for target in (opposite, partner):
            arrival = wide_sem.at[k, len(wide) % 2]
            wide.append(send(rows_v.at[k], wide_v.at[k, t], (WIDE, k), arrival, {"tp": target}))
        wide_v[k, t] = rows_v[k]
    pairs, units = [], []
    for k in range(2):
        loads["cot", k].wait()
        with jax.named_scope(f"coords_wait#k={k}"):
            wait_bytes(coord_v.at[k, pl.ds(0, m - 1)], coord_sem.at[k])
        part = jnp.dot(
            coord_v[k, :, 0].reshape(rank, tokens), cot_v[k], preferred_element_type=jnp.float32
        ) + jnp.dot(coord_v[k, :, 1].reshape(rank, tokens), cot_v[k], preferred_element_type=jnp.float32)
        part_v[k] = part.reshape(n, low_rows, columns)
        code, unit = encode_scaled(part)
        mine_v[k] = code.reshape(n, low_rows, columns)
        unit_v[0, k, 0] = jnp.broadcast_to(unit, unit_v.shape[3:])
        pairs.append({})
        units.append(
            {0: send(unit_v.at[0, k, 0], unit_v.at[1, k, 0], (UNIT, k), unit_sem.at[k, 0], {"fs": across})}
        )
        for d in (*order, 0):
            pairs[k][d] = send(
                mine_v.at[k, along(d, 1 - x)], pair_v.at[k, d], (PAIR, k), pair_sem.at[k, d], {"fs": across}
            )
        advance(pace.pop(0))
    parts = []
    def paired(k, d):
        with jax.named_scope(f"pair_wait#k={k}#d={d}"):
            pairs[k][d].wait_recv()
        return decode(pair_v[k, d]) * unit_v[1, k, 0][:1, :1] + part_v[k, along(d)]

    for k in range(2):
        parts.append({})
        units[k][0].wait_recv()
        for d in order:
            code, unit = encode_scaled(paired(k, d))
            sum_v[k, d] = code
            unit_v[0, k, d] = jnp.broadcast_to(unit, unit_v.shape[3:])
            there = {"fs": along(d)}
            units[k][d] = send(unit_v.at[0, k, d], unit_v.at[1, k, d], (UNIT, k), unit_sem.at[k, d], there)
            parts[k][d] = send(sum_v.at[k, d], got_v.at[k, d], (PART, k), part_sem.at[k, d], there)
        advance(pace.pop(0))

    lows = []
    squares = jnp.zeros((), jnp.float32)
    for k in range(2):
        low = paired(k, 0)
        for d in range(1, half):
            with jax.named_scope(f"part_wait#k={k}#d={d}"):
                units[k][d].wait_recv()
                parts[k][d].wait_recv()
            low = low + decode(got_v[k, d]) * unit_v[1, k, d][:1, :1]
        lows.append(low)
        squares = squares + jnp.sum(low * low)
    square_v[0] = jnp.full(square_v.shape[1:], squares, jnp.float32)
    for d in range(1, n * m):
        other = lax.rem(me + d, n * m)
        there = {"fs": other // m, "tp": lax.rem(other, m)}
        send(square_v.at[0], square_v.at[d], (SQUARE, 0), square_sem, there)
    advance(pace.pop(0))
    for k in range(2):
        loads["first", k].wait()
        loads["second", k].wait()
    with jax.named_scope("square_wait"):
        wait_bytes(square_v.at[pl.ds(1, n * m - 1)], square_sem)
    total_squares = jnp.sum(square_v[...], axis=0)[:1, :1]
    factor = 1.0 / jnp.sqrt(1.0 + total_squares / (2.0 * rank * (columns * m)))

    directions = []
    for k in range(2):
        new_first, new_second, direction = moment_update(lows[k], factor, first[k], second[k])
        direction_v[k, f] = direction
        own = direction_v.at[k, f]
        directions.append(push(own, lambda d: own, DIRECTION, direction_sem, k))
        first_out[k][...] = new_first
        second_out[k][...] = new_second
    advance(pace.pop(0))
    for k in range(2):
        wide[2 * k].wait_recv()
        there = wide_v.at[k, opposite]
        wide.append(send(there, there, (WIDE, k), wide_sem.at[k, 2], {"tp": partner}))
    for k in range(2):
        for d in order:
            with jax.named_scope(f"direction_wait#k={k}#d={d}"):
                directions[k][d].wait_recv()
            there = direction_v.at[k, along(-d)]
            arrival = direction_sem.at[k, half + d]
            directions[k][half + d] = send(there, there, (DIRECTION, k), arrival, {"fs": across})
    advance(pace.pop(0))
    with jax.named_scope("wide_wait"):
        for copy in (wide[1], wide[3], wide[4], wide[5]):
            copy.wait_recv()
    for k in range(2):
        for d in range(1, n):
            flat_v[k, source_of(d)] = wide_v[k, :, d].reshape(rank, block).T
    for k in range(2):
        for d in range(half, n):
            with jax.named_scope(f"direction_late#k={k}#d={d}"):
                directions[k][d].wait_recv()

    def own_rows(k, start, size):
        span = pl.ds(start, size)
        step = jnp.dot(
            basis[k, span, :], direction_v[k].reshape(rank, columns), preferred_element_type=jnp.float32
        )
        weight = master_v[k, span, :] - rate * step
        gathered[k][pl.ds(pl.multiple_of(f * block + start, size), size)] = weight.astype(jnp.bfloat16)
        step_out[k][span] = step
        w_out[k][span] = weight

    def finish(k, s, start, size):
        source = origin[s][k]
        span = pl.ds(start, size)
        step = jnp.dot(
            flat_v[k, source, span, :],
            direction_v[k].reshape(rank, columns),
            preferred_element_type=jnp.float32,
        )
        weight = decode(code_v[k, source, span]) - rate * step
        gathered[k][pl.ds(pl.multiple_of(source * block + start, size), size)] = weight.astype(jnp.bfloat16)

    own = [(k, i * FLIGHT * piece) for i in range(PIECES // FLIGHT) for k in range(2)]
    done = set()

    def ready(limit):
        for s in range(1, n):
            for g in range(PIECES // FLIGHT):
                if limit <= 0:
                    return
                if (s, g) in done or any((s, g * FLIGHT + w) not in arrived for w in range(FLIGHT)):
                    continue
                done.add((s, g))
                limit -= 1
                for k in range(2):
                    finish(k, s, g * FLIGHT * piece, FLIGHT * piece)

    while slots:
        last = slots[0] if slots[0][0] == n - 1 and slots[0][1] >= PIECES - FLIGHT else None
        advance(1)
        if last:
            for k in range(2):
                finish(k, last[0], last[1] * piece, piece)
            done.add((last[0], last[1] // FLIGHT))
        if own:
            k, start = own.pop(0)
            own_rows(k, start, FLIGHT * piece)
        else:
            ready(1)
    for k, start in own:
        own_rows(k, start, FLIGHT * piece)
    ready(n * PIECES)
    with jax.named_scope("drain"):
        for k in range(2):
            wait_bytes(code_v.at[k, pl.ds(0, n - 1)], out_sem.at[RING, k])
            wait_bytes(rows_v.at[k, pl.ds(0, n - 1)], out_sem.at[ROWS, k])
            wait_bytes(coord_v.at[k, pl.ds(0, m - 1)], out_sem.at[COORD, k])
            wait_bytes(wide_v.at[k, pl.ds(0, m - 1)], out_sem.at[WIDE, k])
            wait_bytes(unit_v.at[0, k], out_sem.at[UNIT, k])
            wait_bytes(pair_v.at[k], out_sem.at[PAIR, k])
            wait_bytes(got_v.at[k, pl.ds(1, half - 1)], out_sem.at[PART, k])
            wait_bytes(direction_v.at[k, pl.ds(0, n - 1)], out_sem.at[DIRECTION, k])
        wait_bytes(square_v.at[pl.ds(1, n * m - 1)], out_sem.at[SQUARE, 0])


def write_kernel(count, *refs):
    sem = refs[2 * count]
    copies = [pltpu.make_async_copy(refs[i], refs[count + i], sem.at[i]) for i in range(count)]
    for copy in copies:
        copy.start()
    for copy in copies:
        copy.wait()


def fused_per_device(n, m, *args):
    x, cot, _, _, basis = args[:5]
    first = args[8]
    block, rank = basis.shape
    columns = cot.shape[1]
    tokens, width = x.shape
    part = rank // m
    low_rows = first.shape[0]
    bf16, f32 = jnp.bfloat16, jnp.float32
    kinds = [((block, columns), f32)] * 4 + [(first.shape, f32)] * 4 + [((width, columns), bf16)] * 2
    hbm = pl.BlockSpec(memory_space=pltpu.HBM)
    vmem = pl.BlockSpec(memory_space=pltpu.VMEM)
    dma = pltpu.SemaphoreType.DMA
    results = pl.pallas_call(
        functools.partial(ring_kernel, n, m),
        out_shape=tuple(pltpu.VMEM(*kind) for kind in kinds),
        in_specs=[hbm] * 12,
        out_specs=(vmem,) * 10,
        scratch_shapes=[
            pltpu.VMEM((2, tokens, width), bf16),
            pltpu.VMEM((2, tokens, columns), bf16),
            pltpu.VMEM((2, block, rank), bf16),
            pltpu.VMEM((2, block, columns), f32),
            pltpu.VMEM((2, low_rows, columns), f32),
            pltpu.VMEM((2, low_rows, columns), f32),
            pltpu.VMEM((2, n, part, block), bf16),
            pltpu.VMEM((2, n, block, columns), bf16),
            pltpu.VMEM((2, m, n, part, block), bf16),
            pltpu.VMEM((2, n, block, rank), bf16),
            pltpu.VMEM((2, m, 2, part, tokens), bf16),
            pltpu.VMEM((2, n, low_rows, columns), f32),
            pltpu.VMEM((2, n, low_rows, columns), bf16),
            pltpu.VMEM((2, n // 2, low_rows, columns), bf16),
            pltpu.VMEM((2, n // 2, low_rows, columns), bf16),
            pltpu.VMEM((2, n // 2, low_rows, columns), bf16),
            pltpu.VMEM((2, 2, n // 2, 1, 128), f32),
            pltpu.VMEM((n * m, 1, 128), f32),
            pltpu.VMEM((2, n, low_rows, columns), bf16),
            dma((6, 2)),
            dma((9, 2)),
            dma,
            dma((2,)),
            dma((2, n)),
            dma((2, n // 2)),
            dma((2, n // 2)),
            dma((2, n // 2)),
            dma((2, n)),
            dma((2, n - 1, PIECES)),
            dma((2, 3)),
        ],
        compiler_params=pltpu.CompilerParams(
            collective_id=0, has_side_effects=True, vmem_limit_bytes=48 * 2**20
        ),
    )(*args)
    return pl.pallas_call(
        functools.partial(write_kernel, len(kinds)),
        out_shape=tuple(jax.ShapeDtypeStruct(*kind) for kind in kinds),
        in_specs=[pl.BlockSpec(memory_space=pl.ANY)] * len(kinds),
        out_specs=(hbm,) * len(kinds),
        scratch_shapes=[dma((len(kinds),))],
        compiler_params=pltpu.CompilerParams(vmem_limit_bytes=2**20),
    )(*results)


def fits(n, m, *args):
    basis, first = args[4], args[8]
    return (
        n % 2 == 0
        and m == 4
        and basis.shape[1] // n % 16 == 0
        and basis.shape[1] // m % 16 == 0
        and basis.shape[0] // n % (16 * PIECES) == 0
        and basis.shape[0] // n % 128 == 0
        and first.shape[1] // m % 128 == 0
    )


def solution(mesh):
    placed = (
        P("fs", None),
        P("fs", "tp"),
        P("fs", None),
        P("fs", "tp"),
        P("fs", None),
        P("fs", None),
        P("fs", "tp"),
        P("fs", "tp"),
        P("fs", "tp"),
        P("fs", "tp"),
        P("fs", "tp"),
        P("fs", "tp"),
    )
    n, m = mesh.shape["fs"], mesh.shape["tp"]

    def step(*args):
        body = functools.partial(fused_per_device, n, m) if fits(n, m, *args) else per_device
        return jax.shard_map(
            body,
            mesh=mesh,
            in_specs=placed,
            out_specs=(P("fs", "tp"),) * 8 + (P(None, "tp"),) * 2,
            check_vma=False,
        )(*args)

    return step
```

```python
import functools

import jax
import jax.numpy as jnp
from jax import lax
from jax.experimental import pallas as pl
from jax.experimental.pallas import tpu as pltpu
from jax.sharding import PartitionSpec as P

QW = 2048
RANK = 256


beta_one = 0.8
beta_two = 0.9
rate = 0.1


def moment_update(low, factor, first, second):
    scaled = low * factor
    first_new = beta_one * first + (1.0 - beta_one) * scaled
    second_new = beta_two * second + (1.0 - beta_two) * scaled * scaled
    direction = (first_new / jnp.sqrt(second_new)).astype(jnp.bfloat16)
    return (first_new, second_new, direction)


def contract_tokens(left, right):
    return lax.dot_general(
        left,
        right,
        (((0,), (0,)), ((), ())),
        precision=lax.Precision.HIGHEST,
        preferred_element_type=jnp.float32,
    )


def per_device(
    saved_input,
    query_cotangent,
    layer_cotangent,
    mixed_heads,
    query_basis,
    output_basis,
    query_master,
    output_master,
    query_first,
    query_second,
    output_first,
    output_second,
):
    query_coords = jnp.dot(
        saved_input,
        lax.all_gather(query_basis, "fs", axis=0, tiled=True),
        preferred_element_type=jnp.float32,
    )
    output_coords = jnp.dot(
        layer_cotangent,
        lax.all_gather(output_basis, "fs", axis=0, tiled=True),
        preferred_element_type=jnp.float32,
    )
    query_part = contract_tokens(query_coords, query_cotangent.astype(jnp.float32))
    output_part = contract_tokens(output_coords, mixed_heads.astype(jnp.float32))
    query_low, output_low = (
        lax.psum_scatter(query_part, "fs", scatter_dimension=0, tiled=True),
        lax.psum_scatter(output_part, "fs", scatter_dimension=0, tiled=True),
    )
    local_squares = jnp.sum(query_low * query_low) + jnp.sum(output_low * output_low)
    total_squares = lax.psum(local_squares, ("fs", "tp"))
    factor = 1.0 / jnp.sqrt(1.0 + total_squares / (2.0 * RANK * QW))
    qf, qs, qdir = moment_update(query_low, factor, query_first, query_second)
    of, osec, odir = moment_update(output_low, factor, output_first, output_second)
    query_whole, output_whole = (
        lax.all_gather(qdir, "fs", axis=0, tiled=True),
        lax.all_gather(odir, "fs", axis=0, tiled=True),
    )
    query_step = jnp.dot(query_basis, query_whole, preferred_element_type=jnp.float32)
    output_step = jnp.dot(output_basis, output_whole, preferred_element_type=jnp.float32)
    query_weight = query_master - rate * query_step
    output_weight = output_master - rate * output_step
    query_copy, output_copy = (
        lax.all_gather(query_weight.astype(jnp.bfloat16), "fs", axis=0, tiled=True),
        lax.all_gather(output_weight.astype(jnp.bfloat16), "fs", axis=0, tiled=True),
    )
    return (
        query_weight,
        output_weight,
        query_step,
        output_step,
        qf,
        qs,
        of,
        osec,
        query_copy,
        output_copy,
    )

MESH = pl.DeviceIdType.MESH
PIECES = 8
FLIGHT = 8
PACE = (4, 2, 2, 4, 1, 2, 3, 5, 3, 4, 4, 6, 4, 4)
STRETCH = 40.0
REACH = 3.0
SPLITS = 8
ROWS, COORD, WIDE, UNIT, PAIR, CROSS, SQUARE, DIRECTION, RING = range(9)
LN2 = 0.6931471805599453


def encode(value):
    size = jnp.abs(value) * STRETCH
    small = size * LN2
    near = small * (1.0 + small * (0.5 + small * (1.0 / 6.0)))
    code = jnp.where(small < 0.02, near, jnp.exp2(size) - 1.0)
    return jnp.where(value < 0.0, -code, code).astype(jnp.bfloat16)


def decode(code):
    code = code.astype(jnp.float32)
    size = jnp.abs(code)
    unit = 1.0 / (LN2 * STRETCH)
    value = jnp.where(size < 0.004, size * (unit - size * (0.5 * unit)), jnp.log(1.0 + size) * unit)
    return jnp.where(code < 0.0, -value, value)


def encode_scaled(value):
    peak = jnp.max(jnp.max(jnp.abs(value), axis=1, keepdims=True), axis=0, keepdims=True)
    unit = jnp.maximum(peak, 1e-30) * (1.0 / REACH)
    return encode(value / unit), unit


def ring_kernel(n, m, *refs):
    x_hbm, cot_hbm, basis_hbm, master_hbm, first_hbm, second_hbm = (
        (refs[0], refs[2]),
        (refs[1], refs[3]),
        (refs[4], refs[5]),
        (refs[6], refs[7]),
        (refs[8], refs[10]),
        (refs[9], refs[11]),
    )
    w_out, step_out, first_out, second_out, gathered = (
        (refs[12], refs[13]),
        (refs[14], refs[15]),
        (refs[16], refs[18]),
        (refs[17], refs[19]),
        (refs[20], refs[21]),
    )
    (
        x_v, cot_v, basis, master_v, first, second,
        rows_v, code_v, plain_v, wide_v, flat_v, coord_v, part_v, mine_v, sum_v, got_v, both_v, cross_v, unit_v,
        square_v, direction_v,
        in_sem, out_sem, square_sem, coord_sem, rows_sem, got_sem, cross_sem, unit_sem, direction_sem, ring_sem, wide_sem,
    ) = refs[22:]
    f, t = lax.axis_index("fs"), lax.axis_index("tp")
    me = f * m + t
    rank_part, block = rows_v.shape[2:]
    piece = block // PIECES
    rank = basis.shape[2]
    tokens = x_v.shape[1]
    columns = cot_v.shape[2]
    low_rows = first.shape[1]
    half = n // 2
    z, x = f // 2, lax.rem(f, 2)
    across = z * 2 + 1 - x
    partner, opposite = t + 1 - 2 * lax.rem(t, 2), lax.rem(t + m // 2, m)
    even = lax.rem(z, 2) == 0
    inner = (z > 0) & (z < half - 1)
    outer = jnp.logical_not(inner)
    low_side = z < half // 2
    far, near = jnp.where(low_side, 3, 0), jnp.where(low_side, 2, 1)
    mate = jnp.where(even, z + 1, z - 1)
    reach = (jnp.where(even, 1, 2), jnp.where(low_side, jnp.where(even, 2, 0), jnp.where(even, 3, 1)))
    heard = (*reach, far)

    def column(to):
        return {"fs": to * 2 + x}

    loads = {}
    for i, (name, sources, target) in enumerate(
        (
            ("basis", basis_hbm, basis),
            ("master", master_hbm, master_v),
            ("x", x_hbm, x_v),
            ("cot", cot_hbm, cot_v),
            ("first", first_hbm, first),
            ("second", second_hbm, second),
        )
    ):
        for k in range(2):
            loads[name, k] = pltpu.make_async_copy(sources[k], target.at[k], in_sem.at[i, k])
    for copy in loads.values():
        copy.start()

    barrier = pltpu.get_barrier_semaphore()
    for d in range(1, n * m):
        other = lax.rem(me + d, n * m)
        pl.semaphore_signal(barrier, inc=1, device_id={"fs": other // m, "tp": lax.rem(other, m)}, device_id_type=MESH)

    chosen = lax.broadcasted_iota(jnp.int32, (rank_part, rank), 1) == (
        lax.broadcasted_iota(jnp.int32, (rank_part, rank), 0) + t * rank_part
    )
    select = jnp.where(chosen, 1.0, 0.0).astype(jnp.bfloat16)
    for k in range(2):
        loads["basis", k].wait()
        rows_v[k, f] = lax.dot_general(
            select, basis[k], (((1,), (1,)), ((), ())), preferred_element_type=jnp.float32
        ).astype(jnp.bfloat16)
    with jax.named_scope("barrier"):
        pl.semaphore_wait(barrier, n * m - 1)

    def send(source, target, out, arrival, device):
        copy = pltpu.make_async_remote_copy(
            src_ref=source,
            dst_ref=target,
            send_sem=out_sem.at[out],
            recv_sem=arrival,
            device_id=device,
            device_id_type=MESH,
        )
        copy.start()
        return copy

    def wait_bytes(like, sem):
        pltpu.make_async_copy(like, like, sem).wait()

    def push(block_at, out, sems, k):
        own = block_at(f)
        send(own, own, (out, k), sems.at[k, f], {"fs": across})
        for to in reach:
            send(own, own, (out, k), sems.at[k, f], column(to))

    def arrive(like, sem):
        pltpu.make_async_copy(like, like, sem).wait()

    def relay(block_at, out, sems, k):
        for i, of in enumerate(heard):
            origin_of = of * 2 + x
            there = block_at(origin_of)
            with jax.named_scope(f"relay_wait#o={out}#k={k}#i={i}"):
                arrive(there, sems.at[k, origin_of])
            if i != 1:

                @pl.when(inner)
                def _():
                    send(there, there, (out, k), sems.at[k, origin_of], column(mate))

            send(there, there, (out, k), sems.at[k, origin_of], {"fs": across})

    def late(block_at, out, sems, k):
        for i, of in enumerate((z, *heard)):
            origin_of = of * 2 + 1 - x
            with jax.named_scope(f"late_wait#o={out}#k={k}#i={i}"):
                arrive(block_at(origin_of), sems.at[k, origin_of])

    place = (1 - x) * z + x * (n - 1 - z)

    def at(p):
        p = lax.rem(p + 2 * n, n)
        h = p // half
        return (1 - h) * 2 * p + h * (2 * (n - 1 - p) + 1)

    toward = (at(place + 1), at(place - 1))
    origin = [[at(place - s), at(place + s)] for s in range(n)]
    ring = {}
    slots = [
        (s, g * FLIGHT + w) for g in range(PIECES // FLIGHT) for s in range(n) for w in range(FLIGHT)
    ]
    arrived, fresh = [], []

    def advance(count, relaxed=True):
        for _ in range(min(count, len(slots))):
            s, c = slots.pop(0)
            for k in range(2):
                if s > 0:
                    with jax.named_scope(f"ring_wait#s={s}#c={c}#k={k}"):
                        ring[s - 1, k, c].wait_recv()
                if s < n - 1:
                    where = code_v.at[k, origin[s][k], pl.ds(c * piece, piece)]
                    ring[s, k, c] = send(where, where, (RING, k), ring_sem.at[k, s, c], {"fs": toward[k]})
            if s > 0:
                arrived.append((s, c))
                fresh.append((s, c))
        if relaxed:
            unfold()

    def unfold():
        for s, c in fresh:
            span = pl.ds(c * piece, piece)
            for k in range(2):
                plain_v[k, origin[s][k], span] = decode(code_v[k, origin[s][k], span])
        fresh.clear()

    pace = list(PACE)

    def rows_at(k):
        return lambda of: rows_v.at[k, of]

    for k in range(2):
        push(rows_at(k), ROWS, rows_sem, k)
    for i in range(PIECES // FLIGHT):
        span = pl.ds(i * FLIGHT * piece, FLIGHT * piece)
        for k in range(2):
            if i == 0:
                loads["master", k].wait()
            code_v[k, f, span] = encode(master_v[k, span])
        if i == 0:
            advance(pace.pop(0))

    def coordinates(k, of):
        left = rows_v[k, of]
        right = x_v[k, :, pl.ds(pl.multiple_of(of * block, block), block)]
        return lax.dot_general(left, right, (((1,), (1,)), ((), ())), preferred_element_type=jnp.float32)

    for k in range(2):
        relay(rows_at(k), ROWS, rows_sem, k)
        advance(pace.pop(0))
    for k in range(2):
        loads["x", k].wait()
        total = coordinates(k, f)
        for of in heard:
            total = total + coordinates(k, of * 2 + x)
        late(rows_at(k), ROWS, rows_sem, k)
        for of in (z, *heard):
            total = total + coordinates(k, of * 2 + 1 - x)
        high = total.astype(jnp.bfloat16)
        coord_v[k, t, 0] = high
        coord_v[k, t, 1] = (total - high.astype(jnp.float32)).astype(jnp.bfloat16)
        for d in range(1, m):
            send(coord_v.at[k, t], coord_v.at[k, t], (COORD, k), coord_sem.at[k], {"tp": lax.rem(t + d, m)})
        advance(pace.pop(0))

    wide = []
    for k in range(2):
        for target in (opposite, partner):
            arrival = wide_sem.at[k, len(wide) % 2]
            wide.append(send(rows_v.at[k], wide_v.at[k, t], (WIDE, k), arrival, {"tp": target}))
        wide_v[k, t] = rows_v[k]
    pair_rows = 2 * low_rows

    def ship(k, source, unit, slot, device):
        unit_out, unit_in = unit_v.at[0, k, unit], unit_v.at[1, k, slot]
        send(unit_out, unit_in, (UNIT, k), unit_sem.at[k, slot], device)
        send(source, got_v.at[k, slot], (PAIR, k), got_sem.at[k, slot], device)

    def taken(k, slot):
        with jax.named_scope(f"got_wait#k={k}#slot={slot}"):
            arrive(unit_v.at[1, k, slot], unit_sem.at[k, slot])
            arrive(got_v.at[k, slot], got_sem.at[k, slot])
        return decode(got_v[k, slot]) * unit_v[1, k, slot][:1, :1]

    for k in range(2):
        loads["cot", k].wait()
        with jax.named_scope(f"coords_wait#k={k}"):
            wait_bytes(coord_v.at[k, pl.ds(0, m - 1)], coord_sem.at[k])
        part = jnp.dot(
            coord_v[k, :, 0].reshape(rank, tokens), cot_v[k], preferred_element_type=jnp.float32
        ) + jnp.dot(coord_v[k, :, 1].reshape(rank, tokens), cot_v[k], preferred_element_type=jnp.float32)
        part_v[k] = part.reshape(half, pair_rows, columns)
        code, unit = encode_scaled(part)
        mine_v[k] = code.reshape(half, pair_rows, columns)
        unit_v[0, k, 0] = jnp.broadcast_to(unit, unit_v.shape[3:])

        @pl.when(outer)
        def _():
            ship(k, mine_v.at[k, far], 0, 0, column(mate))
            ship(k, mine_v.at[k, near], 0, 1, column(mate))

        ship(k, mine_v.at[k, mate], 0, 2, column(mate))
        advance(pace.pop(0))
    for k in range(2):

        @pl.when(inner)
        def _():
            for slot, to in enumerate((far, near)):
                code, unit = encode_scaled(taken(k, slot) + part_v[k, to])
                sum_v[k, slot] = code
                unit_v[0, k, 1 + slot] = jnp.broadcast_to(unit, unit_v.shape[3:])
                ship(k, sum_v.at[k, slot], 1 + slot, 3, column(to))

        advance(pace.pop(0))
    for k in range(2):
        both = part_v[k, z] + taken(k, 2) + taken(k, 3)
        both_v[k] = both.reshape(2, low_rows, columns)
        code, unit = encode_scaled(both_v[k, 1 - x])
        cross_v[k, 0] = code
        unit_v[0, k, 3] = jnp.broadcast_to(unit, unit_v.shape[3:])
        there = {"fs": across}
        send(unit_v.at[0, k, 3], unit_v.at[1, k, 4], (UNIT, k), unit_sem.at[k, 4], there)
        send(cross_v.at[k, 0], cross_v.at[k, 1], (CROSS, k), cross_sem.at[k], there)
        advance(pace.pop(0))

    for k in range(2):
        wide[2 * k].wait_recv()
        there = wide_v.at[k, opposite]
        wide.append(send(there, there, (WIDE, k), wide_sem.at[k, 2], {"tp": partner}))
    lows = []
    squares = jnp.zeros((), jnp.float32)
    for k in range(2):
        with jax.named_scope(f"cross_wait#k={k}"):
            arrive(unit_v.at[1, k, 4], unit_sem.at[k, 4])
            arrive(cross_v.at[k, 1], cross_sem.at[k])
        low = both_v[k, x] + decode(cross_v[k, 1]) * unit_v[1, k, 4][:1, :1]
        lows.append(low)
        squares = squares + jnp.sum(low * low)
    square_v[0] = jnp.full(square_v.shape[1:], squares, jnp.float32)
    for d in range(1, n * m):
        other = lax.rem(me + d, n * m)
        there = {"fs": other // m, "tp": lax.rem(other, m)}
        send(square_v.at[0], square_v.at[d], (SQUARE, 0), square_sem, there)
    advance(pace.pop(0))
    with jax.named_scope("wide_wait"):
        for copy in (wide[1], wide[3], wide[4], wide[5]):
            copy.wait_recv()
    for k in range(2):
        for d in range(1, n):
            of = lax.rem(f + d, n)
            flat_v[k, of] = wide_v[k, :, of].reshape(rank, block).T
    for k in range(2):
        loads["first", k].wait()
        loads["second", k].wait()
    with jax.named_scope("square_wait"):
        wait_bytes(square_v.at[pl.ds(1, n * m - 1)], square_sem)
    total_squares = jnp.sum(square_v[...], axis=0)[:1, :1]
    factor = 1.0 / jnp.sqrt(1.0 + total_squares / (2.0 * rank * (columns * m)))

    def directions_at(k):
        return lambda of: direction_v.at[k, of]

    for k in range(2):
        new_first, new_second, direction = moment_update(lows[k], factor, first[k], second[k])
        direction_v[k, f] = direction
        push(directions_at(k), DIRECTION, direction_sem, k)
        first_out[k][...] = new_first
        second_out[k][...] = new_second
    advance(pace.pop(0))
    for k in range(2):
        relay(directions_at(k), DIRECTION, direction_sem, k)
    advance(pace.pop(0))
    for k in range(2):
        late(directions_at(k), DIRECTION, direction_sem, k)

    def own_rows(k, start, size):
        span = pl.ds(start, size)
        step = jnp.dot(
            basis[k, span, :], direction_v[k].reshape(rank, columns), preferred_element_type=jnp.float32
        )
        weight = master_v[k, span, :] - rate * step
        gathered[k][pl.ds(pl.multiple_of(f * block + start, size), size)] = weight.astype(jnp.bfloat16)
        step_out[k][span] = step
        w_out[k][span] = weight

    def finish(k, s, start, size):
        source = origin[s][k]
        span = pl.ds(start, size)
        step = jnp.dot(
            flat_v[k, source, span, :],
            direction_v[k].reshape(rank, columns),
            preferred_element_type=jnp.float32,
        )
        weight = plain_v[k, source, span] - rate * step
        gathered[k][pl.ds(pl.multiple_of(source * block + start, size), size)] = weight.astype(jnp.bfloat16)

    own = [(k, i * FLIGHT * piece) for i in range(PIECES // FLIGHT) for k in range(2)]
    done = set()

    def ready(limit):
        for s in range(1, n):
            for g in range(PIECES // FLIGHT):
                if limit <= 0:
                    return
                if (s, g) in done or any((s, g * FLIGHT + w) not in arrived for w in range(FLIGHT)):
                    continue
                done.add((s, g))
                limit -= 1
                for k in range(2):
                    finish(k, s, g * FLIGHT * piece, FLIGHT * piece)

    while slots:
        last = slots[0] if slots[0][0] == n - 1 and slots[0][1] >= PIECES - FLIGHT else None
        advance(1)
        if last:
            for k in range(2):
                finish(k, last[0], last[1] * piece, piece)
            done.add((last[0], last[1] // FLIGHT))
        if own:
            k, start = own.pop(0)
            own_rows(k, start, FLIGHT * piece)
        else:
            ready(1)
    for k, start in own:
        own_rows(k, start, FLIGHT * piece)
    ready(n * PIECES)
    with jax.named_scope("drain"):
        for k in range(2):
            wait_bytes(code_v.at[k, pl.ds(0, n - 1)], out_sem.at[RING, k])
            for ref, out in ((rows_v, ROWS), (direction_v, DIRECTION)):

                @pl.when(inner)
                def _():
                    wait_bytes(ref.at[k, pl.ds(0, 8)], out_sem.at[out, k])

                @pl.when(outer)
                def _():
                    wait_bytes(ref.at[k, pl.ds(0, 6)], out_sem.at[out, k])

            wait_bytes(coord_v.at[k, pl.ds(0, m - 1)], out_sem.at[COORD, k])
            wait_bytes(wide_v.at[k, pl.ds(0, m - 1)], out_sem.at[WIDE, k])
            wait_bytes(unit_v.at[0, k, pl.ds(0, 4)], out_sem.at[UNIT, k])
            wait_bytes(got_v.at[k, pl.ds(0, 3)], out_sem.at[PAIR, k])
            wait_bytes(cross_v.at[k, 0], out_sem.at[CROSS, k])
        wait_bytes(square_v.at[pl.ds(1, n * m - 1)], out_sem.at[SQUARE, 0])


def write_kernel(count, *refs):
    sem = refs[2 * count]
    copies = []
    for i in reversed(range(count)):
        rows = refs[i].shape[0]
        span = rows // SPLITS if rows % (SPLITS * 16) == 0 else rows
        for start in range(0, rows, span):
            part = pl.ds(start, span)
            copies.append(pltpu.make_async_copy(refs[i].at[part], refs[count + i].at[part], sem.at[i]))
            copies[-1].start()
    for i in range(count):
        pltpu.make_async_copy(refs[i], refs[count + i], sem.at[i]).wait()


def fused_per_device(n, m, *args):
    x, cot, _, _, basis = args[:5]
    first = args[8]
    block, rank = basis.shape
    columns = cot.shape[1]
    tokens, width = x.shape
    part = rank // m
    low_rows = first.shape[0]
    bf16, f32 = jnp.bfloat16, jnp.float32
    kinds = [((block, columns), f32)] * 4 + [(first.shape, f32)] * 4 + [((width, columns), bf16)] * 2
    hbm = pl.BlockSpec(memory_space=pltpu.HBM)
    vmem = pl.BlockSpec(memory_space=pltpu.VMEM)
    dma = pltpu.SemaphoreType.DMA
    results = pl.pallas_call(
        functools.partial(ring_kernel, n, m),
        out_shape=tuple(pltpu.VMEM(*kind) for kind in kinds),
        in_specs=[hbm] * 12,
        out_specs=(vmem,) * 10,
        scratch_shapes=[
            pltpu.VMEM((2, tokens, width), bf16),
            pltpu.VMEM((2, tokens, columns), bf16),
            pltpu.VMEM((2, block, rank), bf16),
            pltpu.VMEM((2, block, columns), f32),
            pltpu.VMEM((2, low_rows, columns), f32),
            pltpu.VMEM((2, low_rows, columns), f32),
            pltpu.VMEM((2, n, part, block), bf16),
            pltpu.VMEM((2, n, block, columns), bf16),
            pltpu.VMEM((2, n, block, columns), f32),
            pltpu.VMEM((2, m, n, part, block), bf16),
            pltpu.VMEM((2, n, block, rank), bf16),
            pltpu.VMEM((2, m, 2, part, tokens), bf16),
            pltpu.VMEM((2, n // 2, 2 * low_rows, columns), f32),
            pltpu.VMEM((2, n // 2, 2 * low_rows, columns), bf16),
            pltpu.VMEM((2, 2, 2 * low_rows, columns), bf16),
            pltpu.VMEM((2, 4, 2 * low_rows, columns), bf16),
            pltpu.VMEM((2, 2, low_rows, columns), f32),
            pltpu.VMEM((2, 2, low_rows, columns), bf16),
            pltpu.VMEM((2, 2, 5, 1, 128), f32),
            pltpu.VMEM((n * m, 1, 128), f32),
            pltpu.VMEM((2, n, low_rows, columns), bf16),
            dma((6, 2)),
            dma((9, 2)),
            dma,
            dma((2,)),
            dma((2, n)),
            dma((2, 4)),
            dma((2,)),
            dma((2, 5)),
            dma((2, n)),
            dma((2, n - 1, PIECES)),
            dma((2, 3)),
        ],
        compiler_params=pltpu.CompilerParams(
            collective_id=0, has_side_effects=True, vmem_limit_bytes=50 * 2**20
        ),
    )(*args)
    return pl.pallas_call(
        functools.partial(write_kernel, len(kinds)),
        out_shape=tuple(jax.ShapeDtypeStruct(*kind) for kind in kinds),
        in_specs=[pl.BlockSpec(memory_space=pl.ANY)] * len(kinds),
        out_specs=(hbm,) * len(kinds),
        scratch_shapes=[dma((len(kinds),))],
        compiler_params=pltpu.CompilerParams(vmem_limit_bytes=2**20),
    )(*results)


def fits(n, m, *args):
    basis, first = args[4], args[8]
    return (
        n == 8
        and m == 4
        and basis.shape[1] // n % 16 == 0
        and basis.shape[1] // m % 16 == 0
        and basis.shape[0] // n % (16 * PIECES) == 0
        and basis.shape[0] // n % 128 == 0
        and first.shape[1] // m % 128 == 0
    )


def solution(mesh):
    placed = (
        P("fs", None),
        P("fs", "tp"),
        P("fs", None),
        P("fs", "tp"),
        P("fs", None),
        P("fs", None),
        P("fs", "tp"),
        P("fs", "tp"),
        P("fs", "tp"),
        P("fs", "tp"),
        P("fs", "tp"),
        P("fs", "tp"),
    )
    n, m = mesh.shape["fs"], mesh.shape["tp"]

    def step(*args):
        body = functools.partial(fused_per_device, n, m) if fits(n, m, *args) else per_device
        return jax.shard_map(
            body,
            mesh=mesh,
            in_specs=placed,
            out_specs=(P("fs", "tp"),) * 8 + (P(None, "tp"),) * 2,
            check_vma=False,
        )(*args)

    return step
```

```python
import functools

import jax
import jax.numpy as jnp
from jax import lax
from jax.experimental import pallas as pl
from jax.experimental.pallas import tpu as pltpu
from jax.sharding import PartitionSpec as P

QW = 2048
RANK = 256


beta_one = 0.8
beta_two = 0.9
rate = 0.1


def moment_update(low, factor, first, second):
    scaled = low * factor
    first_new = beta_one * first + (1.0 - beta_one) * scaled
    second_new = beta_two * second + (1.0 - beta_two) * scaled * scaled
    direction = (first_new / jnp.sqrt(second_new)).astype(jnp.bfloat16)
    return (first_new, second_new, direction)


def contract_tokens(left, right):
    return lax.dot_general(
        left,
        right,
        (((0,), (0,)), ((), ())),
        precision=lax.Precision.HIGHEST,
        preferred_element_type=jnp.float32,
    )


def per_device(
    saved_input,
    query_cotangent,
    layer_cotangent,
    mixed_heads,
    query_basis,
    output_basis,
    query_master,
    output_master,
    query_first,
    query_second,
    output_first,
    output_second,
):
    query_coords = jnp.dot(
        saved_input,
        lax.all_gather(query_basis, "fs", axis=0, tiled=True),
        preferred_element_type=jnp.float32,
    )
    output_coords = jnp.dot(
        layer_cotangent,
        lax.all_gather(output_basis, "fs", axis=0, tiled=True),
        preferred_element_type=jnp.float32,
    )
    query_part = contract_tokens(query_coords, query_cotangent.astype(jnp.float32))
    output_part = contract_tokens(output_coords, mixed_heads.astype(jnp.float32))
    query_low, output_low = (
        lax.psum_scatter(query_part, "fs", scatter_dimension=0, tiled=True),
        lax.psum_scatter(output_part, "fs", scatter_dimension=0, tiled=True),
    )
    local_squares = jnp.sum(query_low * query_low) + jnp.sum(output_low * output_low)
    total_squares = lax.psum(local_squares, ("fs", "tp"))
    factor = 1.0 / jnp.sqrt(1.0 + total_squares / (2.0 * RANK * QW))
    qf, qs, qdir = moment_update(query_low, factor, query_first, query_second)
    of, osec, odir = moment_update(output_low, factor, output_first, output_second)
    query_whole, output_whole = (
        lax.all_gather(qdir, "fs", axis=0, tiled=True),
        lax.all_gather(odir, "fs", axis=0, tiled=True),
    )
    query_step = jnp.dot(query_basis, query_whole, preferred_element_type=jnp.float32)
    output_step = jnp.dot(output_basis, output_whole, preferred_element_type=jnp.float32)
    query_weight = query_master - rate * query_step
    output_weight = output_master - rate * output_step
    query_copy, output_copy = (
        lax.all_gather(query_weight.astype(jnp.bfloat16), "fs", axis=0, tiled=True),
        lax.all_gather(output_weight.astype(jnp.bfloat16), "fs", axis=0, tiled=True),
    )
    return (
        query_weight,
        output_weight,
        query_step,
        output_step,
        qf,
        qs,
        of,
        osec,
        query_copy,
        output_copy,
    )

MESH = pl.DeviceIdType.MESH
PIECES = 8
FLIGHT = 8
PACE = (3, 2, 2, 4, 2, 3, 2, 5, 3, 4, 4, 7, 4, 4)
STRETCH = 40.0
REACH = 3.0
SPLITS = 8
ROWS, COORD, WIDE, UNIT, PAIR, CROSS, SQUARE, DIRECTION, RING, SHIFT = range(10)
SHIFTED = ((DIRECTION, 0), (DIRECTION, 1))
LN2 = 0.6931471805599453


def encode(value):
    size = jnp.abs(value) * STRETCH
    small = size * LN2
    near = small * (1.0 + small * (0.5 + small * (1.0 / 6.0)))
    code = jnp.where(small < 0.02, near, jnp.exp2(size) - 1.0)
    return jnp.where(value < 0.0, -code, code).astype(jnp.bfloat16)


def decode(code):
    code = code.astype(jnp.float32)
    size = jnp.abs(code)
    unit = 1.0 / (LN2 * STRETCH)
    value = jnp.where(size < 0.004, size * (unit - size * (0.5 * unit)), jnp.log(1.0 + size) * unit)
    return jnp.where(code < 0.0, -value, value)


def encode_scaled(value):
    peak = jnp.max(jnp.max(jnp.abs(value), axis=1, keepdims=True), axis=0, keepdims=True)
    unit = jnp.maximum(peak, 1e-30) * (1.0 / REACH)
    return encode(value / unit), unit


def ring_kernel(n, m, *refs):
    x_hbm, cot_hbm, basis_hbm, master_hbm, first_hbm, second_hbm = (
        (refs[0], refs[2]),
        (refs[1], refs[3]),
        (refs[4], refs[5]),
        (refs[6], refs[7]),
        (refs[8], refs[10]),
        (refs[9], refs[11]),
    )
    w_out, step_out, first_out, second_out, gathered = (
        (refs[12], refs[13]),
        (refs[14], refs[15]),
        (refs[16], refs[18]),
        (refs[17], refs[19]),
        (refs[20], refs[21]),
    )
    (
        x_v, cot_v, basis, master_v, first, second,
        rows_v, code_v, plain_v, wide_v, flat_v, coord_v, part_v, mine_v, sum_v, got_v, both_v, cross_v, unit_v,
        square_v, direction_v,
        in_sem, out_sem, square_sem, coord_sem, rows_sem, got_sem, cross_sem, unit_sem, direction_sem, ring_sem, wide_sem,
    ) = refs[22:]
    f, t = lax.axis_index("fs"), lax.axis_index("tp")
    me = f * m + t
    rank_part, block = rows_v.shape[2:]
    piece = block // PIECES
    rank = basis.shape[2]
    tokens = x_v.shape[1]
    columns = cot_v.shape[2]
    low_rows = first.shape[1]
    half = n // 2
    z, x = f // 2, lax.rem(f, 2)
    across = z * 2 + 1 - x
    partner, opposite = t + 1 - 2 * lax.rem(t, 2), lax.rem(t + m // 2, m)
    even = lax.rem(z, 2) == 0
    inner = (z > 0) & (z < half - 1)
    outer = jnp.logical_not(inner)
    low_side = z < half // 2
    far, near = jnp.where(low_side, 3, 0), jnp.where(low_side, 2, 1)
    mate = jnp.where(even, z + 1, z - 1)
    reach = (jnp.where(even, 1, 2), jnp.where(low_side, jnp.where(even, 2, 0), jnp.where(even, 3, 1)))
    heard = (*reach, far)

    def column(to):
        return {"fs": to * 2 + x}

    loads = {}
    for i, (name, sources, target) in enumerate(
        (
            ("basis", basis_hbm, basis),
            ("master", master_hbm, master_v),
            ("x", x_hbm, x_v),
            ("cot", cot_hbm, cot_v),
            ("first", first_hbm, first),
            ("second", second_hbm, second),
        )
    ):
        for k in range(2):
            loads[name, k] = pltpu.make_async_copy(sources[k], target.at[k], in_sem.at[i, k])
    for copy in loads.values():
        copy.start()

    barrier = pltpu.get_barrier_semaphore()
    for d in range(1, n * m):
        other = lax.rem(me + d, n * m)
        pl.semaphore_signal(barrier, inc=1, device_id={"fs": other // m, "tp": lax.rem(other, m)}, device_id_type=MESH)

    chosen = lax.broadcasted_iota(jnp.int32, (rank_part, rank), 1) == (
        lax.broadcasted_iota(jnp.int32, (rank_part, rank), 0) + t * rank_part
    )
    select = jnp.where(chosen, 1.0, 0.0).astype(jnp.bfloat16)
    for k in range(2):
        loads["basis", k].wait()
        rows_v[k, f] = lax.dot_general(
            select, basis[k], (((1,), (1,)), ((), ())), preferred_element_type=jnp.float32
        ).astype(jnp.bfloat16)
    with jax.named_scope("barrier"):
        pl.semaphore_wait(barrier, n * m - 1)

    def describe(source, target, out, arrival, device):
        return pltpu.make_async_remote_copy(
            src_ref=source,
            dst_ref=target,
            send_sem=out_sem.at[out],
            recv_sem=arrival,
            device_id=device,
            device_id_type=MESH,
        )

    def send(*args):
        copy = describe(*args)
        copy.start()
        return copy

    def wait_bytes(like, sem):
        pltpu.make_async_copy(like, like, sem).wait()

    def push(block_at, out, sems, k):
        own = block_at(f)
        send(own, own, (out, k), sems.at[k, f], {"fs": across})
        for to in reach:
            send(own, own, (out, k), sems.at[k, f], column(to))

    def arrive(like, sem):
        pltpu.make_async_copy(like, like, sem).wait()

    def relay(block_at, out, sems, k):
        for i, of in enumerate(heard):
            origin_of = of * 2 + x
            there = block_at(origin_of)
            with jax.named_scope(f"relay_wait#o={out}#k={k}#i={i}"):
                arrive(there, sems.at[k, origin_of])
            if i != 1:

                @pl.when(inner)
                def _():
                    send(there, there, (out, k), sems.at[k, origin_of], column(mate))

            relayed = describe(there, there, (out, k), sems.at[k, origin_of], {"fs": across})
            if i == 2 and (out, k) in SHIFTED:
                pl.when(inner)(relayed.start)
            else:
                relayed.start()

    def late(block_at, out, sems, k):
        for i, of in enumerate((far, z, *reach)):
            origin_of = of * 2 + 1 - x
            there = block_at(origin_of)
            with jax.named_scope(f"late_wait#o={out}#k={k}#i={i}"):
                arrive(there, sems.at[k, origin_of])
            if i == 0 and (out, k) in SHIFTED:
                onward = describe(there, there, (SHIFT + (out == ROWS), k), sems.at[k, origin_of], column(mate))
                pl.when(inner)(onward.start)

    place = (1 - x) * z + x * (n - 1 - z)

    def at(p):
        p = lax.rem(p + 2 * n, n)
        h = p // half
        return (1 - h) * 2 * p + h * (2 * (n - 1 - p) + 1)

    toward = (at(place + 1), at(place - 1))
    origin = [[at(place - s), at(place + s)] for s in range(n)]
    ring = {}
    slots = [
        (s, g * FLIGHT + w) for g in range(PIECES // FLIGHT) for s in range(n) for w in range(FLIGHT)
    ]
    arrived, fresh = [], []

    def advance(count, relaxed=True):
        for _ in range(min(count, len(slots))):
            s, c = slots.pop(0)
            for k in range(2):
                if s > 0:
                    with jax.named_scope(f"ring_wait#s={s}#c={c}#k={k}"):
                        ring[s - 1, k, c].wait_recv()
                if s < n - 1:
                    where = code_v.at[k, origin[s][k], pl.ds(c * piece, piece)]
                    ring[s, k, c] = send(where, where, (RING, k), ring_sem.at[k, s, c], {"fs": toward[k]})
            if s > 0:
                arrived.append((s, c))
                fresh.append((s, c))
        if relaxed:
            unfold()

    def unfold():
        for s, c in fresh:
            span = pl.ds(c * piece, piece)
            for k in range(2):
                plain_v[k, origin[s][k], span] = decode(code_v[k, origin[s][k], span])
        fresh.clear()

    pace = list(PACE)

    def rows_at(k):
        return lambda of: rows_v.at[k, of]

    for k in range(2):
        push(rows_at(k), ROWS, rows_sem, k)
    for i in range(PIECES // FLIGHT):
        span = pl.ds(i * FLIGHT * piece, FLIGHT * piece)
        for k in range(2):
            if i == 0:
                loads["master", k].wait()
            code_v[k, f, span] = encode(master_v[k, span])
        if i == 0:
            advance(pace.pop(0))

    def coordinates(k, of):
        left = rows_v[k, of]
        right = x_v[k, :, pl.ds(pl.multiple_of(of * block, block), block)]
        return lax.dot_general(left, right, (((1,), (1,)), ((), ())), preferred_element_type=jnp.float32)

    for k in range(2):
        relay(rows_at(k), ROWS, rows_sem, k)
        advance(pace.pop(0))
    for k in range(2):
        loads["x", k].wait()
        total = coordinates(k, f)
        for of in heard:
            total = total + coordinates(k, of * 2 + x)
        late(rows_at(k), ROWS, rows_sem, k)
        for of in (z, *heard):
            total = total + coordinates(k, of * 2 + 1 - x)
        high = total.astype(jnp.bfloat16)
        coord_v[k, t, 0] = high
        coord_v[k, t, 1] = (total - high.astype(jnp.float32)).astype(jnp.bfloat16)
        for d in range(1, m):
            send(coord_v.at[k, t], coord_v.at[k, t], (COORD, k), coord_sem.at[k], {"tp": lax.rem(t + d, m)})
        advance(pace.pop(0))

    wide = []
    for k in range(2):
        for target in (opposite, partner):
            arrival = wide_sem.at[k, len(wide) % 2]
            wide.append(send(rows_v.at[k], wide_v.at[k, t], (WIDE, k), arrival, {"tp": target}))
        wide_v[k, t] = rows_v[k]
    pair_rows = 2 * low_rows

    def ship(k, source, unit, slot, device):
        unit_out, unit_in = unit_v.at[0, k, unit], unit_v.at[1, k, slot]
        send(unit_out, unit_in, (UNIT, k), unit_sem.at[k, slot], device)
        send(source, got_v.at[k, slot], (PAIR, k), got_sem.at[k, slot], device)

    def taken(k, slot):
        with jax.named_scope(f"got_wait#k={k}#slot={slot}"):
            arrive(unit_v.at[1, k, slot], unit_sem.at[k, slot])
            arrive(got_v.at[k, slot], got_sem.at[k, slot])
        return decode(got_v[k, slot]) * unit_v[1, k, slot][:1, :1]

    for k in range(2):
        loads["cot", k].wait()
        with jax.named_scope(f"coords_wait#k={k}"):
            wait_bytes(coord_v.at[k, pl.ds(0, m - 1)], coord_sem.at[k])
        part = jnp.dot(
            coord_v[k, :, 0].reshape(rank, tokens), cot_v[k], preferred_element_type=jnp.float32
        ) + jnp.dot(coord_v[k, :, 1].reshape(rank, tokens), cot_v[k], preferred_element_type=jnp.float32)
        part_v[k] = part.reshape(half, pair_rows, columns)
        code, unit = encode_scaled(part)
        mine_v[k] = code.reshape(half, pair_rows, columns)
        unit_v[0, k, 0] = jnp.broadcast_to(unit, unit_v.shape[3:])

        @pl.when(outer)
        def _():
            ship(k, mine_v.at[k, far], 0, 0, column(mate))
            ship(k, mine_v.at[k, near], 0, 1, column(mate))

            ship(k, mine_v.at[k, mate], 0, 2, column(mate))

        advance(pace.pop(0))
    for k in range(2):

        @pl.when(inner)
        def _():
            for slot, to in enumerate((far, near)):
                code, unit = encode_scaled(taken(k, slot) + part_v[k, to])
                sum_v[k, slot] = code
                unit_v[0, k, 1 + slot] = jnp.broadcast_to(unit, unit_v.shape[3:])
                ship(k, sum_v.at[k, slot], 1 + slot, 4 - slot, column(near))

        advance(pace.pop(0))
    for k in range(2):

        @pl.when(inner)
        def _():
            code, unit = encode_scaled(taken(k, 4) + part_v[k, mate])
            sum_v[k, 2] = code
            unit_v[0, k, 4] = jnp.broadcast_to(unit, unit_v.shape[3:])
            ship(k, sum_v.at[k, 2], 4, 2, column(mate))
            part_v[k, z] = part_v[k, z] + taken(k, 3)

        both = part_v[k, z] + taken(k, 2)
        both_v[k] = both.reshape(2, low_rows, columns)
        code, unit = encode_scaled(both_v[k, 1 - x])
        cross_v[k, 0] = code
        unit_v[0, k, 3] = jnp.broadcast_to(unit, unit_v.shape[3:])
        there = {"fs": across}
        send(unit_v.at[0, k, 3], unit_v.at[1, k, 5], (UNIT, k), unit_sem.at[k, 5], there)
        send(cross_v.at[k, 0], cross_v.at[k, 1], (CROSS, k), cross_sem.at[k], there)
        advance(pace.pop(0))

    for k in range(2):
        wide[2 * k].wait_recv()
        there = wide_v.at[k, opposite]
        wide.append(send(there, there, (WIDE, k), wide_sem.at[k, 2], {"tp": partner}))
    lows = []
    squares = jnp.zeros((), jnp.float32)
    for k in range(2):
        with jax.named_scope(f"cross_wait#k={k}"):
            arrive(unit_v.at[1, k, 5], unit_sem.at[k, 5])
            arrive(cross_v.at[k, 1], cross_sem.at[k])
        low = both_v[k, x] + decode(cross_v[k, 1]) * unit_v[1, k, 5][:1, :1]
        lows.append(low)
        squares = squares + jnp.sum(low * low)
    square_v[0] = jnp.full(square_v.shape[1:], squares, jnp.float32)
    for d in range(1, n * m):
        other = lax.rem(me + d, n * m)
        there = {"fs": other // m, "tp": lax.rem(other, m)}
        send(square_v.at[0], square_v.at[d], (SQUARE, 0), square_sem, there)
    advance(pace.pop(0))
    with jax.named_scope("wide_wait"):
        for copy in (wide[1], wide[3], wide[4], wide[5]):
            copy.wait_recv()
    for k in range(2):
        for d in range(1, n):
            of = lax.rem(f + d, n)
            flat_v[k, of] = wide_v[k, :, of].reshape(rank, block).T
    for k in range(2):
        loads["first", k].wait()
        loads["second", k].wait()
    with jax.named_scope("square_wait"):
        wait_bytes(square_v.at[pl.ds(1, n * m - 1)], square_sem)
    total_squares = jnp.sum(square_v[...], axis=0)[:1, :1]
    factor = 1.0 / jnp.sqrt(1.0 + total_squares / (2.0 * rank * (columns * m)))

    def directions_at(k):
        return lambda of: direction_v.at[k, of]

    for k in range(2):
        new_first, new_second, direction = moment_update(lows[k], factor, first[k], second[k])
        direction_v[k, f] = direction
        push(directions_at(k), DIRECTION, direction_sem, k)
        first_out[k][...] = new_first
        second_out[k][...] = new_second
    advance(pace.pop(0))
    for k in range(2):
        relay(directions_at(k), DIRECTION, direction_sem, k)
    advance(pace.pop(0))
    for k in range(2):
        late(directions_at(k), DIRECTION, direction_sem, k)

    def own_rows(k, start, size):
        span = pl.ds(start, size)
        step = jnp.dot(
            basis[k, span, :], direction_v[k].reshape(rank, columns), preferred_element_type=jnp.float32
        )
        weight = master_v[k, span, :] - rate * step
        gathered[k][pl.ds(pl.multiple_of(f * block + start, size), size)] = weight.astype(jnp.bfloat16)
        step_out[k][span] = step
        w_out[k][span] = weight

    def finish(k, s, start, size):
        source = origin[s][k]
        span = pl.ds(start, size)
        step = jnp.dot(
            flat_v[k, source, span, :],
            direction_v[k].reshape(rank, columns),
            preferred_element_type=jnp.float32,
        )
        weight = plain_v[k, source, span] - rate * step
        gathered[k][pl.ds(pl.multiple_of(source * block + start, size), size)] = weight.astype(jnp.bfloat16)

    own = [(k, i * FLIGHT * piece) for i in range(PIECES // FLIGHT) for k in range(2)]
    done = set()

    def ready(limit):
        for s in range(1, n):
            for g in range(PIECES // FLIGHT):
                if limit <= 0:
                    return
                if (s, g) in done or any((s, g * FLIGHT + w) not in arrived for w in range(FLIGHT)):
                    continue
                done.add((s, g))
                limit -= 1
                for k in range(2):
                    finish(k, s, g * FLIGHT * piece, FLIGHT * piece)

    while slots:
        last = slots[0] if slots[0][0] == n - 1 and slots[0][1] >= PIECES - FLIGHT else None
        advance(1)
        if last:
            for k in range(2):
                finish(k, last[0], last[1] * piece, piece)
            done.add((last[0], last[1] // FLIGHT))
        if own:
            k, start = own.pop(0)
            own_rows(k, start, FLIGHT * piece)
        else:
            ready(1)
    for k, start in own:
        own_rows(k, start, FLIGHT * piece)
    ready(n * PIECES)
    with jax.named_scope("drain"):
        for k in range(2):
            wait_bytes(code_v.at[k, pl.ds(0, n - 1)], out_sem.at[RING, k])
            for ref, out in ((rows_v, ROWS), (direction_v, DIRECTION)):

                @pl.when(inner)
                def _():
                    wait_bytes(ref.at[k, pl.ds(0, 8)], out_sem.at[out, k])

                @pl.when(outer)
                def _():
                    wait_bytes(ref.at[k, pl.ds(0, 5 if (out, k) in SHIFTED else 6)], out_sem.at[out, k])

                if (out, k) in SHIFTED:

                    @pl.when(inner)
                    def _():
                        wait_bytes(ref.at[k, 0], out_sem.at[SHIFT + (out == ROWS), k])

            wait_bytes(coord_v.at[k, pl.ds(0, m - 1)], out_sem.at[COORD, k])
            wait_bytes(wide_v.at[k, pl.ds(0, m - 1)], out_sem.at[WIDE, k])
            wait_bytes(unit_v.at[0, k, pl.ds(0, 4)], out_sem.at[UNIT, k])
            wait_bytes(got_v.at[k, pl.ds(0, 3)], out_sem.at[PAIR, k])
            wait_bytes(cross_v.at[k, 0], out_sem.at[CROSS, k])
        wait_bytes(square_v.at[pl.ds(1, n * m - 1)], out_sem.at[SQUARE, 0])


def write_kernel(count, *refs):
    sem = refs[2 * count]
    copies = []
    for i in reversed(range(count)):
        rows = refs[i].shape[0]
        span = rows // SPLITS if rows % (SPLITS * 16) == 0 else rows
        for start in range(0, rows, span):
            part = pl.ds(start, span)
            copies.append(pltpu.make_async_copy(refs[i].at[part], refs[count + i].at[part], sem.at[i]))
            copies[-1].start()
    for i in range(count):
        pltpu.make_async_copy(refs[i], refs[count + i], sem.at[i]).wait()


def fused_per_device(n, m, *args):
    x, cot, _, _, basis = args[:5]
    first = args[8]
    block, rank = basis.shape
    columns = cot.shape[1]
    tokens, width = x.shape
    part = rank // m
    low_rows = first.shape[0]
    bf16, f32 = jnp.bfloat16, jnp.float32
    kinds = [((block, columns), f32)] * 4 + [(first.shape, f32)] * 4 + [((width, columns), bf16)] * 2
    hbm = pl.BlockSpec(memory_space=pltpu.HBM)
    vmem = pl.BlockSpec(memory_space=pltpu.VMEM)
    dma = pltpu.SemaphoreType.DMA
    results = pl.pallas_call(
        functools.partial(ring_kernel, n, m),
        out_shape=tuple(pltpu.VMEM(*kind) for kind in kinds),
        in_specs=[hbm] * 12,
        out_specs=(vmem,) * 10,
        scratch_shapes=[
            pltpu.VMEM((2, tokens, width), bf16),
            pltpu.VMEM((2, tokens, columns), bf16),
            pltpu.VMEM((2, block, rank), bf16),
            pltpu.VMEM((2, block, columns), f32),
            pltpu.VMEM((2, low_rows, columns), f32),
            pltpu.VMEM((2, low_rows, columns), f32),
            pltpu.VMEM((2, n, part, block), bf16),
            pltpu.VMEM((2, n, block, columns), bf16),
            pltpu.VMEM((2, n, block, columns), f32),
            pltpu.VMEM((2, m, n, part, block), bf16),
            pltpu.VMEM((2, n, block, rank), bf16),
            pltpu.VMEM((2, m, 2, part, tokens), bf16),
            pltpu.VMEM((2, n // 2, 2 * low_rows, columns), f32),
            pltpu.VMEM((2, n // 2, 2 * low_rows, columns), bf16),
            pltpu.VMEM((2, 3, 2 * low_rows, columns), bf16),
            pltpu.VMEM((2, 5, 2 * low_rows, columns), bf16),
            pltpu.VMEM((2, 2, low_rows, columns), f32),
            pltpu.VMEM((2, 2, low_rows, columns), bf16),
            pltpu.VMEM((2, 2, 6, 1, 128), f32),
            pltpu.VMEM((n * m, 1, 128), f32),
            pltpu.VMEM((2, n, low_rows, columns), bf16),
            dma((6, 2)),
            dma((11, 2)),
            dma,
            dma((2,)),
            dma((2, n)),
            dma((2, 5)),
            dma((2,)),
            dma((2, 6)),
            dma((2, n)),
            dma((2, n - 1, PIECES)),
            dma((2, 3)),
        ],
        compiler_params=pltpu.CompilerParams(
            collective_id=0, has_side_effects=True, vmem_limit_bytes=50 * 2**20
        ),
    )(*args)
    return pl.pallas_call(
        functools.partial(write_kernel, len(kinds)),
        out_shape=tuple(jax.ShapeDtypeStruct(*kind) for kind in kinds),
        in_specs=[pl.BlockSpec(memory_space=pl.ANY)] * len(kinds),
        out_specs=(hbm,) * len(kinds),
        scratch_shapes=[dma((len(kinds),))],
        compiler_params=pltpu.CompilerParams(vmem_limit_bytes=2**20),
    )(*results)


def fits(n, m, *args):
    basis, first = args[4], args[8]
    return (
        n == 8
        and m == 4
        and basis.shape[1] // n % 16 == 0
        and basis.shape[1] // m % 16 == 0
        and basis.shape[0] // n % (16 * PIECES) == 0
        and basis.shape[0] // n % 128 == 0
        and first.shape[1] // m % 128 == 0
    )


def solution(mesh):
    placed = (
        P("fs", None),
        P("fs", "tp"),
        P("fs", None),
        P("fs", "tp"),
        P("fs", None),
        P("fs", None),
        P("fs", "tp"),
        P("fs", "tp"),
        P("fs", "tp"),
        P("fs", "tp"),
        P("fs", "tp"),
        P("fs", "tp"),
    )
    n, m = mesh.shape["fs"], mesh.shape["tp"]

    def step(*args):
        body = functools.partial(fused_per_device, n, m) if fits(n, m, *args) else per_device
        return jax.shard_map(
            body,
            mesh=mesh,
            in_specs=placed,
            out_specs=(P("fs", "tp"),) * 8 + (P(None, "tp"),) * 2,
            check_vma=False,
        )(*args)

    return step
```

```python
import functools

import jax
import jax.numpy as jnp
from jax import lax
from jax.experimental import pallas as pl
from jax.experimental.pallas import tpu as pltpu
from jax.sharding import PartitionSpec as P

QW = 2048
RANK = 256


beta_one = 0.8
beta_two = 0.9
rate = 0.1


def moment_update(low, factor, first, second):
    scaled = low * factor
    first_new = beta_one * first + (1.0 - beta_one) * scaled
    second_new = beta_two * second + (1.0 - beta_two) * scaled * scaled
    direction = (first_new / jnp.sqrt(second_new)).astype(jnp.bfloat16)
    return (first_new, second_new, direction)


def contract_tokens(left, right):
    return lax.dot_general(
        left,
        right,
        (((0,), (0,)), ((), ())),
        precision=lax.Precision.HIGHEST,
        preferred_element_type=jnp.float32,
    )


def per_device(
    saved_input,
    query_cotangent,
    layer_cotangent,
    mixed_heads,
    query_basis,
    output_basis,
    query_master,
    output_master,
    query_first,
    query_second,
    output_first,
    output_second,
):
    query_coords = jnp.dot(
        saved_input,
        lax.all_gather(query_basis, "fs", axis=0, tiled=True),
        preferred_element_type=jnp.float32,
    )
    output_coords = jnp.dot(
        layer_cotangent,
        lax.all_gather(output_basis, "fs", axis=0, tiled=True),
        preferred_element_type=jnp.float32,
    )
    query_part = contract_tokens(query_coords, query_cotangent.astype(jnp.float32))
    output_part = contract_tokens(output_coords, mixed_heads.astype(jnp.float32))
    query_low, output_low = (
        lax.psum_scatter(query_part, "fs", scatter_dimension=0, tiled=True),
        lax.psum_scatter(output_part, "fs", scatter_dimension=0, tiled=True),
    )
    local_squares = jnp.sum(query_low * query_low) + jnp.sum(output_low * output_low)
    total_squares = lax.psum(local_squares, ("fs", "tp"))
    factor = 1.0 / jnp.sqrt(1.0 + total_squares / (2.0 * RANK * QW))
    qf, qs, qdir = moment_update(query_low, factor, query_first, query_second)
    of, osec, odir = moment_update(output_low, factor, output_first, output_second)
    query_whole, output_whole = (
        lax.all_gather(qdir, "fs", axis=0, tiled=True),
        lax.all_gather(odir, "fs", axis=0, tiled=True),
    )
    query_step = jnp.dot(query_basis, query_whole, preferred_element_type=jnp.float32)
    output_step = jnp.dot(output_basis, output_whole, preferred_element_type=jnp.float32)
    query_weight = query_master - rate * query_step
    output_weight = output_master - rate * output_step
    query_copy, output_copy = (
        lax.all_gather(query_weight.astype(jnp.bfloat16), "fs", axis=0, tiled=True),
        lax.all_gather(output_weight.astype(jnp.bfloat16), "fs", axis=0, tiled=True),
    )
    return (
        query_weight,
        output_weight,
        query_step,
        output_step,
        qf,
        qs,
        of,
        osec,
        query_copy,
        output_copy,
    )

MESH = pl.DeviceIdType.MESH
PIECES = 8
FLIGHT = 8
PACE = (3, 2, 2, 4, 2, 3, 2, 5, 3, 4, 4, 7, 4, 4)
STRETCH = 40.0
REACH = 3.0
SPLITS = 8
ROWS, COORD, WIDE, UNIT, PAIR, CROSS, SQUARE, DIRECTION, RING, SHIFT = range(10)
SHIFTED = ((DIRECTION, 0), (DIRECTION, 1))
LN2 = 0.6931471805599453


def encode(value):
    size = jnp.abs(value) * STRETCH
    small = size * LN2
    near = small * (1.0 + small * (0.5 + small * (1.0 / 6.0)))
    code = jnp.where(small < 0.02, near, jnp.exp2(size) - 1.0)
    return jnp.where(value < 0.0, -code, code).astype(jnp.bfloat16)


def decode(code):
    code = code.astype(jnp.float32)
    size = jnp.abs(code)
    unit = 1.0 / (LN2 * STRETCH)
    value = jnp.where(size < 0.004, size * (unit - size * (0.5 * unit)), jnp.log(1.0 + size) * unit)
    return jnp.where(code < 0.0, -value, value)


def encode_scaled(value):
    peak = jnp.max(jnp.max(jnp.abs(value), axis=1, keepdims=True), axis=0, keepdims=True)
    unit = jnp.maximum(peak, 1e-30) * (1.0 / REACH)
    return encode(value / unit), unit


def ring_kernel(n, m, *refs):
    x_hbm, cot_hbm, basis_hbm, master_hbm, first_hbm, second_hbm = (
        (refs[0], refs[2]),
        (refs[1], refs[3]),
        (refs[4], refs[5]),
        (refs[6], refs[7]),
        (refs[8], refs[10]),
        (refs[9], refs[11]),
    )
    w_out, step_out, first_out, second_out, gathered = (
        (refs[12], refs[13]),
        (refs[14], refs[15]),
        (refs[16], refs[18]),
        (refs[17], refs[19]),
        (refs[20], refs[21]),
    )
    (
        x_v, cot_v, basis, master_v, first, second,
        rows_v, code_v, plain_v, wide_v, flat_v, coord_v, part_v, mine_v, sum_v, got_v, both_v, cross_v, unit_v,
        square_v, direction_v,
        in_sem, out_sem, square_sem, coord_sem, rows_sem, got_sem, cross_sem, unit_sem, ring_sem, wide_sem,
    ) = refs[22:]
    f, t = lax.axis_index("fs"), lax.axis_index("tp")
    me = f * m + t
    rank_part, block = rows_v.shape[2:]
    piece = block // PIECES
    rank = basis.shape[2]
    tokens = x_v.shape[1]
    columns = cot_v.shape[2]
    low_rows = first.shape[1]
    half = n // 2
    z, x = f // 2, lax.rem(f, 2)
    across = z * 2 + 1 - x
    partner, opposite = t + 1 - 2 * lax.rem(t, 2), lax.rem(t + m // 2, m)
    even = lax.rem(z, 2) == 0
    inner = (z > 0) & (z < half - 1)
    outer = jnp.logical_not(inner)
    low_side = z < half // 2
    far, near = jnp.where(low_side, 3, 0), jnp.where(low_side, 2, 1)
    mate = jnp.where(even, z + 1, z - 1)
    reach = (jnp.where(even, 1, 2), jnp.where(low_side, jnp.where(even, 2, 0), jnp.where(even, 3, 1)))
    heard = (*reach, far)

    def column(to):
        return {"fs": to * 2 + x}

    loads = {}
    for i, (name, sources, target) in enumerate(
        (
            ("basis", basis_hbm, basis),
            ("master", master_hbm, master_v),
            ("x", x_hbm, x_v),
            ("cot", cot_hbm, cot_v),
            ("first", first_hbm, first),
            ("second", second_hbm, second),
        )
    ):
        for k in range(2):
            loads[name, k] = pltpu.make_async_copy(sources[k], target.at[k], in_sem.at[i, k])
    for copy in loads.values():
        copy.start()

    barrier = pltpu.get_barrier_semaphore()
    for d in range(1, n * m):
        other = lax.rem(me + d, n * m)
        pl.semaphore_signal(barrier, inc=1, device_id={"fs": other // m, "tp": lax.rem(other, m)}, device_id_type=MESH)

    chosen = lax.broadcasted_iota(jnp.int32, (rank_part, rank), 1) == (
        lax.broadcasted_iota(jnp.int32, (rank_part, rank), 0) + t * rank_part
    )
    select = jnp.where(chosen, 1.0, 0.0).astype(jnp.bfloat16)
    for k in range(2):
        loads["basis", k].wait()
        rows_v[k, f] = lax.dot_general(
            select, basis[k], (((1,), (1,)), ((), ())), preferred_element_type=jnp.float32
        ).astype(jnp.bfloat16)
    with jax.named_scope("barrier"):
        pl.semaphore_wait(barrier, n * m - 1)

    def describe(source, target, out, arrival, device):
        return pltpu.make_async_remote_copy(
            src_ref=source,
            dst_ref=target,
            send_sem=out_sem.at[out],
            recv_sem=arrival,
            device_id=device,
            device_id_type=MESH,
        )

    def send(*args):
        copy = describe(*args)
        copy.start()
        return copy

    def wait_bytes(like, sem):
        pltpu.make_async_copy(like, like, sem).wait()

    def push(block_at, out, sems, k):
        own = block_at(f)
        send(own, own, (out, k), sems.at[k, f], {"fs": across})
        for to in reach:
            send(own, own, (out, k), sems.at[k, f], column(to))

    def arrive(like, sem):
        pltpu.make_async_copy(like, like, sem).wait()

    def relay(block_at, out, sems, k):
        for i, of in enumerate(heard):
            origin_of = of * 2 + x
            there = block_at(origin_of)
            with jax.named_scope(f"relay_wait#o={out}#k={k}#i={i}"):
                arrive(there, sems.at[k, origin_of])
            if i != 1:

                @pl.when(inner)
                def _():
                    send(there, there, (out, k), sems.at[k, origin_of], column(mate))

            relayed = describe(there, there, (out, k), sems.at[k, origin_of], {"fs": across})
            if i == 2 and (out, k) in SHIFTED:
                pl.when(inner)(relayed.start)
            else:
                relayed.start()

    def late(block_at, out, sems, k):
        for i, of in enumerate((far, z, *reach)):
            origin_of = of * 2 + 1 - x
            there = block_at(origin_of)
            with jax.named_scope(f"late_wait#o={out}#k={k}#i={i}"):
                arrive(there, sems.at[k, origin_of])
            if i == 0 and (out, k) in SHIFTED:
                onward = describe(there, there, (SHIFT + (out == ROWS), k), sems.at[k, origin_of], column(mate))
                pl.when(inner)(onward.start)

    place = (1 - x) * z + x * (n - 1 - z)

    def at(p):
        p = lax.rem(p + 2 * n, n)
        h = p // half
        return (1 - h) * 2 * p + h * (2 * (n - 1 - p) + 1)

    toward = (at(place + 1), at(place - 1))
    origin = [[at(place - s), at(place + s)] for s in range(n)]
    ring = {}
    slots = [
        (s, g * FLIGHT + w) for g in range(PIECES // FLIGHT) for s in range(n) for w in range(FLIGHT)
    ]
    arrived, fresh = [], []
    slot_of, waited, spare = {}, ([], []), ([], [])
    fresh_slot = {(s, k, c): i for i, (s, c) in enumerate(slots) if s < n - 1 for k in range(2)}

    def advance(count, relaxed=True):
        for _ in range(min(count, len(slots))):
            s, c = slots.pop(0)
            for k in range(2):
                if s > 0:
                    with jax.named_scope(f"ring_wait#s={s}#c={c}#k={k}"):
                        ring[s - 1, k, c].wait_recv()
                        waited[k].append(slot_of[s - 1, k, c])
                if s < n - 1:
                    where = code_v.at[k, origin[s][k], pl.ds(c * piece, piece)]
                    slot = spare[k].pop(0) if spare[k] else fresh_slot.pop((s, k, c))
                    slot_of[s, k, c] = slot
                    ring[s, k, c] = send(where, where, (RING, k), ring_sem.at[k, slot], {"fs": toward[k]})
            if s > 0:
                arrived.append((s, c))
                fresh.append((s, c))
        if relaxed:
            unfold()

    def unfold():
        for s, c in fresh:
            span = pl.ds(c * piece, piece)
            for k in range(2):
                plain_v[k, origin[s][k], span] = decode(code_v[k, origin[s][k], span])
        fresh.clear()

    pace = list(PACE)

    def rows_at(k):
        return lambda of: rows_v.at[k, of]

    for k in range(2):
        push(rows_at(k), ROWS, rows_sem, k)
    for i in range(PIECES // FLIGHT):
        span = pl.ds(i * FLIGHT * piece, FLIGHT * piece)
        for k in range(2):
            if i == 0:
                loads["master", k].wait()
            code_v[k, f, span] = encode(master_v[k, span])
        if i == 0:
            advance(pace.pop(0))

    def coordinates(k, of):
        left = rows_v[k, of]
        right = x_v[k, :, pl.ds(pl.multiple_of(of * block, block), block)]
        return lax.dot_general(left, right, (((1,), (1,)), ((), ())), preferred_element_type=jnp.float32)

    for k in range(2):
        relay(rows_at(k), ROWS, rows_sem, k)
        advance(pace.pop(0))
    for k in range(2):
        loads["x", k].wait()
        total = coordinates(k, f)
        for of in heard:
            total = total + coordinates(k, of * 2 + x)
        late(rows_at(k), ROWS, rows_sem, k)
        for of in (z, *heard):
            total = total + coordinates(k, of * 2 + 1 - x)
        high = total.astype(jnp.bfloat16)
        coord_v[k, t, 0] = high
        coord_v[k, t, 1] = (total - high.astype(jnp.float32)).astype(jnp.bfloat16)
        for d in range(1, m):
            send(coord_v.at[k, t], coord_v.at[k, t], (COORD, k), coord_sem.at[k], {"tp": lax.rem(t + d, m)})
        advance(pace.pop(0))

    wide = []
    for k in range(2):
        for target in (opposite, partner):
            arrival = wide_sem.at[k, len(wide) % 2]
            wide.append(send(rows_v.at[k], wide_v.at[k, t], (WIDE, k), arrival, {"tp": target}))
        wide_v[k, t] = rows_v[k]
    pair_rows = 2 * low_rows

    def ship(k, source, unit, slot, device):
        unit_out, unit_in = unit_v.at[0, k, unit], unit_v.at[1, k, slot]
        send(unit_out, unit_in, (UNIT, k), unit_sem.at[k, slot], device)
        send(source, got_v.at[k, slot], (PAIR, k), got_sem.at[k, slot], device)

    def taken(k, slot):
        with jax.named_scope(f"got_wait#k={k}#slot={slot}"):
            arrive(unit_v.at[1, k, slot], unit_sem.at[k, slot])
            arrive(got_v.at[k, slot], got_sem.at[k, slot])
        return decode(got_v[k, slot]) * unit_v[1, k, slot][:1, :1]

    for k in range(2):
        loads["cot", k].wait()
        with jax.named_scope(f"coords_wait#k={k}"):
            wait_bytes(coord_v.at[k, pl.ds(0, m - 1)], coord_sem.at[k])
        part = jnp.dot(
            coord_v[k, :, 0].reshape(rank, tokens), cot_v[k], preferred_element_type=jnp.float32
        ) + jnp.dot(coord_v[k, :, 1].reshape(rank, tokens), cot_v[k], preferred_element_type=jnp.float32)
        part_v[k] = part.reshape(half, pair_rows, columns)
        code, unit = encode_scaled(part)
        mine_v[k] = code.reshape(half, pair_rows, columns)
        unit_v[0, k, 0] = jnp.broadcast_to(unit, unit_v.shape[3:])

        @pl.when(outer)
        def _():
            ship(k, mine_v.at[k, far], 0, 0, column(mate))
            ship(k, mine_v.at[k, near], 0, 1, column(mate))

            ship(k, mine_v.at[k, mate], 0, 2, column(mate))

        advance(pace.pop(0))
    for k in range(2):

        @pl.when(inner)
        def _():
            for slot, to in enumerate((far, near)):
                code, unit = encode_scaled(taken(k, slot) + part_v[k, to])
                sum_v[k, slot] = code
                unit_v[0, k, 1 + slot] = jnp.broadcast_to(unit, unit_v.shape[3:])
                ship(k, sum_v.at[k, slot], 1 + slot, 4 - slot, column(near))

        advance(pace.pop(0))
    for k in range(2):

        @pl.when(inner)
        def _():
            code, unit = encode_scaled(taken(k, 4) + part_v[k, mate])
            sum_v[k, 2] = code
            unit_v[0, k, 4] = jnp.broadcast_to(unit, unit_v.shape[3:])
            ship(k, sum_v.at[k, 2], 4, 2, column(mate))
            part_v[k, z] = part_v[k, z] + taken(k, 3)

        both = part_v[k, z] + taken(k, 2)
        both_v[k] = both.reshape(2, low_rows, columns)
        code, unit = encode_scaled(both_v[k, 1 - x])
        cross_v[k, 0] = code
        unit_v[0, k, 3] = jnp.broadcast_to(unit, unit_v.shape[3:])
        there = {"fs": across}
        send(unit_v.at[0, k, 3], unit_v.at[1, k, 5], (UNIT, k), unit_sem.at[k, 5], there)
        send(cross_v.at[k, 0], cross_v.at[k, 1], (CROSS, k), cross_sem.at[k], there)
        advance(pace.pop(0))

    for k in range(2):
        wide[2 * k].wait_recv()
        there = wide_v.at[k, opposite]
        wide.append(send(there, there, (WIDE, k), wide_sem.at[k, 2], {"tp": partner}))
    lows = []
    squares = jnp.zeros((), jnp.float32)
    for k in range(2):
        with jax.named_scope(f"cross_wait#k={k}"):
            arrive(unit_v.at[1, k, 5], unit_sem.at[k, 5])
            arrive(cross_v.at[k, 1], cross_sem.at[k])
        low = both_v[k, x] + decode(cross_v[k, 1]) * unit_v[1, k, 5][:1, :1]
        lows.append(low)
        squares = squares + jnp.sum(low * low)
    settled = [list(indices) for indices in waited]
    square_v[0] = jnp.full(square_v.shape[1:], squares, jnp.float32)
    for d in range(1, n * m):
        other = lax.rem(me + d, n * m)
        there = {"fs": other // m, "tp": lax.rem(other, m)}
        send(square_v.at[0], square_v.at[d], (SQUARE, 0), square_sem, there)
    advance(pace.pop(0))
    with jax.named_scope("wide_wait"):
        for copy in (wide[1], wide[3], wide[4], wide[5]):
            copy.wait_recv()
    for k in range(2):
        for d in range(1, n):
            of = lax.rem(f + d, n)
            flat_v[k, of] = wide_v[k, :, of].reshape(rank, block).T
    for k in range(2):
        loads["first", k].wait()
        loads["second", k].wait()
    with jax.named_scope("square_wait"):
        wait_bytes(square_v.at[pl.ds(1, n * m - 1)], square_sem)
    for k in range(2):
        spare[k].extend(settled[k])
    total_squares = jnp.sum(square_v[...], axis=0)[:1, :1]
    factor = 1.0 / jnp.sqrt(1.0 + total_squares / (2.0 * rank * (columns * m)))

    def directions_at(k):
        return lambda of: direction_v.at[k, of]

    for k in range(2):
        new_first, new_second, direction = moment_update(lows[k], factor, first[k], second[k])
        direction_v[k, f] = direction
        push(directions_at(k), DIRECTION, rows_sem, k)
        first_out[k][...] = new_first
        second_out[k][...] = new_second
    advance(pace.pop(0))
    for k in range(2):
        relay(directions_at(k), DIRECTION, rows_sem, k)
    advance(pace.pop(0))
    for k in range(2):
        late(directions_at(k), DIRECTION, rows_sem, k)

    def own_rows(k, start, size):
        span = pl.ds(start, size)
        step = jnp.dot(
            basis[k, span, :], direction_v[k].reshape(rank, columns), preferred_element_type=jnp.float32
        )
        weight = master_v[k, span, :] - rate * step
        gathered[k][pl.ds(pl.multiple_of(f * block + start, size), size)] = weight.astype(jnp.bfloat16)
        step_out[k][span] = step
        w_out[k][span] = weight

    def finish(k, s, start, size):
        source = origin[s][k]
        span = pl.ds(start, size)
        step = jnp.dot(
            flat_v[k, source, span, :],
            direction_v[k].reshape(rank, columns),
            preferred_element_type=jnp.float32,
        )
        weight = plain_v[k, source, span] - rate * step
        gathered[k][pl.ds(pl.multiple_of(source * block + start, size), size)] = weight.astype(jnp.bfloat16)

    own = [(k, i * FLIGHT * piece) for i in range(PIECES // FLIGHT) for k in range(2)]
    done = set()

    def ready(limit):
        for s in range(1, n):
            for g in range(PIECES // FLIGHT):
                if limit <= 0:
                    return
                if (s, g) in done or any((s, g * FLIGHT + w) not in arrived for w in range(FLIGHT)):
                    continue
                done.add((s, g))
                limit -= 1
                for k in range(2):
                    finish(k, s, g * FLIGHT * piece, FLIGHT * piece)

    while slots:
        last = slots[0] if slots[0][0] == n - 1 and slots[0][1] >= PIECES - FLIGHT else None
        advance(1)
        if last:
            for k in range(2):
                finish(k, last[0], last[1] * piece, piece)
            done.add((last[0], last[1] // FLIGHT))
        if own:
            k, start = own.pop(0)
            own_rows(k, start, FLIGHT * piece)
        else:
            ready(1)
    for k, start in own:
        own_rows(k, start, FLIGHT * piece)
    ready(n * PIECES)
    with jax.named_scope("drain"):
        for k in range(2):
            wait_bytes(code_v.at[k, pl.ds(0, n - 1)], out_sem.at[RING, k])
            for ref, out in ((rows_v, ROWS), (direction_v, DIRECTION)):

                @pl.when(inner)
                def _():
                    wait_bytes(ref.at[k, pl.ds(0, 8)], out_sem.at[out, k])

                @pl.when(outer)
                def _():
                    wait_bytes(ref.at[k, pl.ds(0, 5 if (out, k) in SHIFTED else 6)], out_sem.at[out, k])

                if (out, k) in SHIFTED:

                    @pl.when(inner)
                    def _():
                        wait_bytes(ref.at[k, 0], out_sem.at[SHIFT + (out == ROWS), k])

            wait_bytes(coord_v.at[k, pl.ds(0, m - 1)], out_sem.at[COORD, k])
            wait_bytes(wide_v.at[k, pl.ds(0, m - 1)], out_sem.at[WIDE, k])
            wait_bytes(unit_v.at[0, k, pl.ds(0, 4)], out_sem.at[UNIT, k])
            wait_bytes(got_v.at[k, pl.ds(0, 3)], out_sem.at[PAIR, k])
            wait_bytes(cross_v.at[k, 0], out_sem.at[CROSS, k])
        wait_bytes(square_v.at[pl.ds(1, n * m - 1)], out_sem.at[SQUARE, 0])


def write_kernel(count, *refs):
    sem = refs[2 * count]
    copies = []
    for i in reversed(range(count)):
        rows = refs[i].shape[0]
        span = rows // SPLITS if rows % (SPLITS * 16) == 0 else rows
        for start in range(0, rows, span):
            part = pl.ds(start, span)
            copies.append(pltpu.make_async_copy(refs[i].at[part], refs[count + i].at[part], sem.at[i]))
            copies[-1].start()
    for i in range(count):
        pltpu.make_async_copy(refs[i], refs[count + i], sem.at[i]).wait()


def fused_per_device(n, m, *args):
    x, cot, _, _, basis = args[:5]
    first = args[8]
    block, rank = basis.shape
    columns = cot.shape[1]
    tokens, width = x.shape
    part = rank // m
    low_rows = first.shape[0]
    bf16, f32 = jnp.bfloat16, jnp.float32
    kinds = [((block, columns), f32)] * 4 + [(first.shape, f32)] * 4 + [((width, columns), bf16)] * 2
    hbm = pl.BlockSpec(memory_space=pltpu.HBM)
    vmem = pl.BlockSpec(memory_space=pltpu.VMEM)
    dma = pltpu.SemaphoreType.DMA
    results = pl.pallas_call(
        functools.partial(ring_kernel, n, m),
        out_shape=tuple(pltpu.VMEM(*kind) for kind in kinds),
        in_specs=[hbm] * 12,
        out_specs=(vmem,) * 10,
        scratch_shapes=[
            pltpu.VMEM((2, tokens, width), bf16),
            pltpu.VMEM((2, tokens, columns), bf16),
            pltpu.VMEM((2, block, rank), bf16),
            pltpu.VMEM((2, block, columns), f32),
            pltpu.VMEM((2, low_rows, columns), f32),
            pltpu.VMEM((2, low_rows, columns), f32),
            pltpu.VMEM((2, n, part, block), bf16),
            pltpu.VMEM((2, n, block, columns), bf16),
            pltpu.VMEM((2, n, block, columns), f32),
            pltpu.VMEM((2, m, n, part, block), bf16),
            pltpu.VMEM((2, n, block, rank), bf16),
            pltpu.VMEM((2, m, 2, part, tokens), bf16),
            pltpu.VMEM((2, n // 2, 2 * low_rows, columns), f32),
            pltpu.VMEM((2, n // 2, 2 * low_rows, columns), bf16),
            pltpu.VMEM((2, 3, 2 * low_rows, columns), bf16),
            pltpu.VMEM((2, 5, 2 * low_rows, columns), bf16),
            pltpu.VMEM((2, 2, low_rows, columns), f32),
            pltpu.VMEM((2, 2, low_rows, columns), bf16),
            pltpu.VMEM((2, 2, 6, 1, 128), f32),
            pltpu.VMEM((n * m, 1, 128), f32),
            pltpu.VMEM((2, n, low_rows, columns), bf16),
            dma((6, 2)),
            dma((11, 2)),
            dma,
            dma((2,)),
            dma((2, n)),
            dma((2, 5)),
            dma((2,)),
            dma((2, 6)),
            dma((2, min(sum(PACE[:12]), (n - 1) * PIECES))),
            dma((2, 3)),
        ],
        compiler_params=pltpu.CompilerParams(
            collective_id=0, has_side_effects=True, vmem_limit_bytes=50 * 2**20
        ),
    )(*args)
    return pl.pallas_call(
        functools.partial(write_kernel, len(kinds)),
        out_shape=tuple(jax.ShapeDtypeStruct(*kind) for kind in kinds),
        in_specs=[pl.BlockSpec(memory_space=pl.ANY)] * len(kinds),
        out_specs=(hbm,) * len(kinds),
        scratch_shapes=[dma((len(kinds),))],
        compiler_params=pltpu.CompilerParams(vmem_limit_bytes=2**20),
    )(*results)


def fits(n, m, *args):
    basis, first = args[4], args[8]
    return (
        n == 8
        and m == 4
        and basis.shape[1] // n % 16 == 0
        and basis.shape[1] // m % 16 == 0
        and basis.shape[0] // n % (16 * PIECES) == 0
        and basis.shape[0] // n % 128 == 0
        and first.shape[1] // m % 128 == 0
    )


def solution(mesh):
    placed = (
        P("fs", None),
        P("fs", "tp"),
        P("fs", None),
        P("fs", "tp"),
        P("fs", None),
        P("fs", None),
        P("fs", "tp"),
        P("fs", "tp"),
        P("fs", "tp"),
        P("fs", "tp"),
        P("fs", "tp"),
        P("fs", "tp"),
    )
    n, m = mesh.shape["fs"], mesh.shape["tp"]

    def step(*args):
        body = functools.partial(fused_per_device, n, m) if fits(n, m, *args) else per_device
        return jax.shard_map(
            body,
            mesh=mesh,
            in_specs=placed,
            out_specs=(P("fs", "tp"),) * 8 + (P(None, "tp"),) * 2,
            check_vma=False,
        )(*args)

    return step
```
